128 devices in a mesh: ep: 32 (over z, y, core), tp: 4 (over x).
Axes of the slice: x: 4, y: 4, z: 4, core: 2. Of those that a mesh axis runs over, the one named last changes fastest.
Arguments:
- query_rows: bfloat16 [8192, 2048], P('ep', 'tp'), may hold values from -6 to 6
- key_rows: bfloat16 [8192, 512], P('ep', 'tp'), may hold values from -18 to 18
- value_rows: bfloat16 [8192, 512], P('ep', 'tp'), may hold values from -12 to 12
- key_bias: bfloat16 [8192, 8], P('ep', 'tp'), may hold values from -2 to 13
- head_offset: float32 [32], P('tp'), may hold values from -16 to -3
- out_weight: bfloat16 [2048, 2048], P('tp'), may hold values from -0.125 to 0.125
- expert_input: bfloat16 [16384, 2048], P(('ep', 'tp')), may hold values from -40 to 40
- expert_gain: float32 [2048], replicated, may hold values from 0.1 to 1.9
- routes: int32 [16384, 2], P(('ep', 'tp')), may hold values from 0 to 31, all different within a row; in each aligned block of 128 rows (0 to 127, 128 to 255, ...) at most 12 rows name the same one
- route_weight: float32 [16384, 2], P(('ep', 'tp')), may hold values from 0.5 to 2
- gate_weight: bfloat16 [32, 2048, 3584], P('ep', None, 'tp'), may hold values from -0.125 to 0.125
- up_weight: bfloat16 [32, 2048, 3584], P('ep', None, 'tp'), may hold values from -0.125 to 0.125
- down_weight: bfloat16 [32, 3584, 2048], P('ep', 'tp'), may hold values from -0.09375 to 0.09375
Outputs:
- mixed_a: bfloat16 [8192, 2048], P(('ep', 'tp'))
- mixed_b: bfloat16 [16384, 2048], P(('ep', 'tp'))
The draws below stay inside these ranges and needn't reach their ends.
Inputs may be any that keep to these rules, and one draw needn't show every extreme that they name: `routes`: each row names 2 different experts; in the rows of one device (aligned blocks of 128 rows) no expert is named more than 12 times, and in every draw some device names some expert exactly 12 times.
All inputs are finite; a program needn't handle non-finite values.
Results may differ from the reference program's by a relative error of at most 0.012.
Values may be sent and summed in bfloat16 or wider, within the bound.
A program may use at most 128 MiB of HBM per device.

```python
import math
import jax
import jax.numpy as jnp
import numpy as np
from jax import lax

D = 2048
HEADS = 32
KEY_VALUE_HEADS = 8
HD = 64
FF = 3584
TOPK = 2
TOK_A = 256
TOK_B = 128
SEQUENCE_LEN_A = 8192
TOKENS_B = 16384
EXPERTS = 32
CAP = 12
N_EP = 32
N_TP = 4


def draw_head_offset(key, part):
    first_key, second_key, key_third_part = jax.random.split(jax.random.fold_in(key, 17), 3)
    picks = jax.random.randint(first_key, (HEADS,), 0, 8)
    slow_heads = picks < 4
    slow_value = -4.5 - math.log(SEQUENCE_LEN_A) + jax.random.uniform(second_key, (HEADS,), jnp.float32, -0.5, 0.5)
    fast_value = jax.random.uniform(key_third_part, (HEADS,), jnp.float32, -5.0, -3.0)
    return jnp.where(slow_heads, slow_value, fast_value).astype(jnp.float32)


def draw_key_bias(key, part):
    first_key, second_key, key_third_part = jax.random.split(jax.random.fold_in(key, 23), 3)
    spread = 0.8
    block_count = SEQUENCE_LEN_A // TOK_A
    factors = jax.random.uniform(first_key, (block_count, 1, KEY_VALUE_HEADS), jnp.float32, -spread, spread)
    factors = jnp.broadcast_to(factors, (block_count, TOK_A, KEY_VALUE_HEADS)).reshape(SEQUENCE_LEN_A, KEY_VALUE_HEADS)
    noise = 0.3 * jax.random.normal(second_key, (SEQUENCE_LEN_A, KEY_VALUE_HEADS), jnp.float32)
    start_offset = jnp.clip(factors + noise, -1.5, 1.5)
    group_position = jax.random.randint(key_third_part, (2, KEY_VALUE_HEADS), 0, SEQUENCE_LEN_A)
    token_group = jnp.any(jnp.arange(SEQUENCE_LEN_A)[:, None, None] == group_position[None, :, :], axis=1)
    return (start_offset + 11.0 * token_group.astype(jnp.float32)).astype(jnp.bfloat16)


def draw_expert_input(key, part):
    first_key, second_key = jax.random.split(jax.random.fold_in(key, 31), 2)
    scales = jnp.exp(jax.random.uniform(first_key, (TOKENS_B, 1), jnp.float32, 0.0, math.log(10.0)))
    values = jnp.clip(jax.random.normal(second_key, (TOKENS_B, D), jnp.float32), -4.0, 4.0)
    return (values * scales).astype(jnp.bfloat16)


def level_of(stream_key, dims, shards, low, high):
    level, own = 1.0, jax.random.fold_in(stream_key, 6)
    for position, blocks in shards:
        heights = jnp.exp(jax.random.uniform(jax.random.fold_in(own, position), (blocks,), jnp.float32, low / len(shards), high / len(shards)))
        level = level * jnp.repeat(heights, dims[position] // blocks).reshape([-1 if axis == position else 1 for axis in range(len(dims))])
    return level


def shared_out(own_key, own, number, rows, number_of, top, reach, slope):
    sequence = jax.random.permutation(own_key, number_of)
    heavy_load, usual = portions_of(number_of, rows * top, reach, slope, True), portions_of(number_of, rows * top, reach, slope, False)
    places = jnp.arange(number_of)

    def named(tallies, offset_by):
        used = int((tallies > 0).sum())
        fixed = max(1, used // 4)
        moved = fixed + (places - fixed + offset_by * (used - fixed)) % max(1, number_of - fixed)
        return jnp.zeros((number_of,), jnp.int32).at[sequence[jnp.where(places < fixed, places, moved)]].set(jnp.asarray(tallies, jnp.int32))

    tallies = jnp.where(number % 4 == 0, named(heavy_load, number // 4), named(usual, number - number // 4 - 1))
    mixed = jax.random.permutation(jax.random.fold_in(own, 3), number_of)
    source_of, taker = mixed[0:number_of // 2 * 2:2], mixed[1:number_of // 2 * 2:2]
    slack = jnp.minimum(tallies[source_of] - 1, reach - tallies[taker]) // 2
    slack = jnp.where((source_of == sequence[0]) | (taker == sequence[0]) | (tallies[taker] == 0), 0, jnp.maximum(slack, 0))
    moved = jax.random.randint(jax.random.fold_in(own, 4), (number_of // 2,), 0, 1 << 20) % (slack + 1)
    tallies = tallies.at[source_of].add(-moved).at[taker].add(moved)
    items = jnp.searchsorted(jnp.cumsum(tallies), jnp.arange(rows * top), side="right").astype(jnp.int32)
    listing = items.reshape(top, rows).T
    listing = listing[jax.random.permutation(jax.random.fold_in(own, 1), rows)]
    offset_by = jax.random.randint(jax.random.fold_in(own, 2), (rows, 1), 0, top)
    return jnp.take_along_axis(listing, (jnp.arange(top)[None, :] + offset_by) % top, axis=1)


def portions_of(number_of, total, most, slope, full):
    weights = [(1 << 20) // math.isqrt(standing ** slope) + 1 for standing in range(1, number_of + 1)]
    largest = most if full else min(most, max(-(-total // number_of), total * weights[0] // sum(weights)))
    least = 1 if total - largest >= number_of - 1 else 0
    given, surplus = [largest] + [least] * (number_of - 1), total - largest - least * (number_of - 1)
    while surplus > 0:
        free = [i for i in range(1, number_of) if given[i] < largest] or [i for i in range(1, number_of) if given[i] < most]
        pool, remaining = sum([weights[i] for i in free]), surplus
        for i in free:
            addition = min(most - given[i], max(1, remaining * weights[i] // pool), surplus)
            given[i] = given[i] + addition
            surplus = surplus - addition
    return np.array(given)


def normal_values(own_key, extent, scale, reach, cuts=(), kind=jnp.bfloat16):
    entries = jax.random.normal(own_key, extent, jnp.float32) * scale
    if len(cuts) > 0:
        entries = level_of(own_key, extent, cuts, -0.22, 0.18) * entries
    return jnp.clip(entries, min=-reach, max=reach).astype(kind)


def setup_inputs(seed: int = 0) -> dict:
    seeds = jax.random.split(jax.random.key(seed), 14)
    query_rows = normal_values(seeds[0], (SEQUENCE_LEN_A, HEADS * HD), 1.0, 6.0, ((0, 32), (1, 4)))
    key_rows = normal_values(seeds[1], (SEQUENCE_LEN_A, KEY_VALUE_HEADS * HD), 3.0, 18.0, ((0, 32), (1, 4)))
    value_rows = normal_values(seeds[2], (SEQUENCE_LEN_A, KEY_VALUE_HEADS * HD), 2.0, 12.0, ((0, 32), (1, 4)))
    key_bias = draw_key_bias(jax.random.fold_in(seeds[13], 71), 0)
    head_offset = draw_head_offset(jax.random.fold_in(seeds[13], 71), 0)
    out_weight = normal_values(seeds[5], (HEADS * HD, D), (HEADS * HD) ** -0.5, 0.125, ((0, 4),))
    expert_input = draw_expert_input(jax.random.fold_in(seeds[13], 71), 0)
    expert_gain = jnp.clip(1.0 + 0.18 * jax.random.normal(seeds[7], (D,), jnp.float32), 0.1, 1.9)
    routes_keys = jax.random.split(jax.random.fold_in(seeds[8], 1), TOKENS_B // TOK_B)
    routes_turns = jax.random.permutation(jax.random.fold_in(seeds[8], 3), TOKENS_B // TOK_B)
    routes = jax.vmap(lambda own, number: shared_out(jax.random.fold_in(seeds[8], 2), own, number, TOK_B, EXPERTS, TOPK, CAP, 1))(routes_keys, routes_turns).reshape((TOKENS_B, TOPK))
    route_weight = jnp.clip(0.5 + 1.5 * jax.random.uniform(seeds[9], (TOKENS_B, TOPK), jnp.float32) ** level_of(seeds[9], (TOKENS_B, TOPK), ((0, 128),), -0.2, 0.2), 0.5, 2.0)
    gate_weight = normal_values(seeds[10], (EXPERTS, D, FF), D ** -0.5, 0.125, ((0, 32), (2, 4)))
    up_weight = normal_values(seeds[11], (EXPERTS, D, FF), D ** -0.5, 0.125, ((0, 32), (2, 4)))
    down_weight = normal_values(seeds[12], (EXPERTS, FF, D), FF ** -0.5, 0.09375, ((0, 32), (1, 4)))
    return {"query_rows": query_rows, "key_rows": key_rows, "value_rows": value_rows, "key_bias": key_bias, "head_offset": head_offset, "out_weight": out_weight, "expert_input": expert_input, "expert_gain": expert_gain, "routes": routes, "route_weight": route_weight, "gate_weight": gate_weight, "up_weight": up_weight, "down_weight": down_weight}


EPSILON = 1e-06

def rms_normed(rows, gain):
    values = rows.astype(jnp.float32)
    scaled = values * lax.rsqrt(lax.optimization_barrier(jnp.mean(values * values, axis=-1, keepdims=True)) + EPSILON)
    return (scaled * gain).astype(jnp.bfloat16)

def stick_heads(query_rows, key_rows, value_rows, key_bias, head_offset):
    group_size = HEADS // KEY_VALUE_HEADS
    queries4 = query_rows.astype(jnp.float32).reshape(SEQUENCE_LEN_A, KEY_VALUE_HEADS, group_size, HD)
    key_heads = key_rows.astype(jnp.float32).reshape(SEQUENCE_LEN_A, KEY_VALUE_HEADS, HD)
    value_heads = value_rows.astype(jnp.float32).reshape(SEQUENCE_LEN_A, KEY_VALUE_HEADS, HD)
    offsets = head_offset.reshape(KEY_VALUE_HEADS, group_size)
    bias_rows = jnp.transpose(key_bias.astype(jnp.float32))
    block_rows = math.gcd(TOK_A, 128)
    key_pos = jnp.arange(SEQUENCE_LEN_A, dtype=jnp.int32)

    def one_block(block_turn):
        first_row = (block_turn * block_rows).astype(jnp.int32)
        query_block = lax.dynamic_slice_in_dim(queries4, first_row, block_rows, 0)
        scores = jnp.einsum('qgjd,kgd->gjqk', query_block, key_heads) * (1.0 / math.sqrt(HD))
        scores = scores + offsets[:, :, None, None] + bias_rows[:, None, None, :]
        query_pos = first_row + jnp.arange(block_rows, dtype=jnp.int32)
        keep_mask = key_pos[None, :] < query_pos[:, None]
        log_stay = jnp.where(keep_mask, jax.nn.log_sigmoid(-scores), 0.0)
        after_sum = lax.cumsum(log_stay, axis=3, reverse=True) - log_stay
        weights = jnp.where(keep_mask, jnp.exp(jax.nn.log_sigmoid(scores) + after_sum), 0.0).astype(jnp.bfloat16)
        weights = lax.optimization_barrier(weights).astype(jnp.float32)
        return jnp.einsum('gjqk,kgd->qgjd', weights, value_heads).reshape(block_rows, HEADS * HD)
    blocks = lax.map(one_block, jnp.arange(SEQUENCE_LEN_A // block_rows, dtype=jnp.int32))
    return blocks.reshape(SEQUENCE_LEN_A, HEADS * HD).astype(jnp.bfloat16)

def reference(query_rows, key_rows, value_rows, key_bias, head_offset, out_weight, expert_input, expert_gain, routes, route_weight, gate_weight, up_weight, down_weight):
    heads_out = stick_heads(query_rows, key_rows, value_rows, key_bias, head_offset)
    col_part = HEADS * HD // N_TP
    total_sum = jnp.zeros((SEQUENCE_LEN_A, D), jnp.float32)
    for tp_part in range(N_TP):
        lower = tp_part * col_part
        partial_value = jnp.dot(heads_out[:, lower:lower + col_part], out_weight[lower:lower + col_part], preferred_element_type=jnp.float32).astype(jnp.bfloat16)
        total_sum = total_sum + lax.optimization_barrier(partial_value).astype(jnp.float32)
    mixed_a = total_sum.astype(jnp.bfloat16)
    normed = rms_normed(expert_input, expert_gain)
    flat_route = routes.reshape(-1)
    flat_token = (jnp.arange(TOKENS_B * TOPK, dtype=jnp.int32) // TOPK).astype(jnp.int32)
    flattened_weight = route_weight.reshape(-1)
    row_limit = N_EP * N_TP * CAP
    hidden_part = FF // N_TP

    def one_expert(expert_id):
        order_rows = jnp.argsort((flat_route != expert_id).astype(jnp.int32), stable=True)[:row_limit].astype(jnp.int32)
        live = flat_route[order_rows] == expert_id
        inputs = normed[flat_token[order_rows]]
        gate_act = jnp.dot(inputs, gate_weight[expert_id], preferred_element_type=jnp.float32)
        up_act = jnp.dot(inputs, up_weight[expert_id], preferred_element_type=jnp.float32)
        hidden = (jax.nn.silu(gate_act) * up_act).astype(jnp.bfloat16)
        down_rows = down_weight[expert_id]
        expert_sum = jnp.zeros((row_limit, D), jnp.float32)
        for tp_part in range(N_TP):
            lower = tp_part * hidden_part
            partial_value = jnp.dot(hidden[:, lower:lower + hidden_part], down_rows[lower:lower + hidden_part], preferred_element_type=jnp.float32).astype(jnp.bfloat16)
            expert_sum = expert_sum + lax.optimization_barrier(partial_value).astype(jnp.float32)
        result = lax.optimization_barrier(expert_sum.astype(jnp.bfloat16)).astype(jnp.float32)
        scaled = result * jnp.where(live, flattened_weight[order_rows], 0.0)[:, None]
        return (order_rows, scaled)
    orders, results = lax.map(one_expert, jnp.arange(EXPERTS, dtype=jnp.int32))
    combined = jnp.zeros((TOKENS_B, D), jnp.float32).at[flat_token[orders.reshape(-1)]].add(results.reshape(-1, D))
    mixed_b = combined.astype(jnp.bfloat16)
    return (mixed_a, mixed_b)
```

```python
import functools
import math

import jax
import jax.numpy as jnp
from jax import lax
from jax.experimental import pallas as pl
from jax.experimental.pallas import tpu as pltpu
from jax.sharding import PartitionSpec as P

HD = 64
BLK = 256
EPSILON = 1e-06
TO_LOG2 = math.log2(math.e) / math.sqrt(HD)


def rms_normed(rows, gain):
    values = rows.astype(jnp.float32)
    scaled = values * lax.rsqrt(jnp.mean(values * values, axis=-1, keepdims=True) + EPSILON)
    return (scaled * gain).astype(jnp.bfloat16)


def stick_kernel(count_ref, q_ref, kv_ref, o_ref, acc, surv, tri, *, tile):
    count = count_ref[0]
    rows = q_ref.shape[1]
    at_row = lax.broadcasted_iota(jnp.int32, (BLK, BLK), 0)
    at_col = lax.broadcasted_iota(jnp.int32, (BLK, BLK), 1)
    tri[...] = jnp.where(at_row > at_col, -1.0, 0.0).astype(jnp.bfloat16)
    acc[...] = jnp.zeros_like(acc)
    surv[...] = jnp.zeros_like(surv)

    def block(index, diagonal):
        at = pl.multiple_of(index * BLK, BLK)
        keys = kv_ref[pl.ds(at, BLK), 0:256]
        for g in range(2):
            vals = kv_ref[pl.ds(at, BLK), 256 + HD * g : 256 + HD * (g + 1)]
            for m in range(rows // tile):
                part = slice(m * tile, (m + 1) * tile)
                z = (
                    lax.dot_general(
                        q_ref[g, part, :],
                        keys,
                        (((1,), (1,)), ((), ())),
                        preferred_element_type=jnp.float32,
                    )
                    * TO_LOG2
                )
                if diagonal:
                    query = lax.broadcasted_iota(jnp.int32, (tile, BLK), 0) % BLK
                    key = lax.broadcasted_iota(jnp.int32, (tile, BLK), 1)
                    z = jnp.where(key < query, z, -1e30)
                leave = jnp.maximum(z, jnp.log2(1.0 + jnp.exp2(jnp.minimum(z, 100.0))))
                after = (
                    jnp.dot(
                        leave.astype(jnp.bfloat16), tri[...], preferred_element_type=jnp.float32
                    )
                    - leave
                )
                s = surv[g, part, :]
                w = jnp.exp2(z + after + jnp.concatenate([s, s], axis=1)).astype(jnp.bfloat16)
                acc[g, part, :] += jnp.dot(w, vals, preferred_element_type=jnp.float32)
                surv[g, part, :] = s + jnp.broadcast_to(after[:, 0:1], s.shape)

    block(count - 1, True)

    def step(i, _):
        block(count - 2 - i, False)
        return 0

    lax.fori_loop(0, count - 1, step, 0)
    o_ref[...] = acc[...].astype(jnp.bfloat16)


def attention(count, q_aug, kv, tile=512):
    rows = q_aug.shape[1]
    return pl.pallas_call(
        functools.partial(stick_kernel, tile=tile),
        out_shape=jax.ShapeDtypeStruct((2, rows, HD), jnp.bfloat16),
        in_specs=[
            pl.BlockSpec(memory_space=pltpu.SMEM),
            pl.BlockSpec(memory_space=pltpu.VMEM),
            pl.BlockSpec(memory_space=pltpu.VMEM),
        ],
        out_specs=pl.BlockSpec(memory_space=pltpu.VMEM),
        scratch_shapes=[
            pltpu.VMEM((2, rows, HD), jnp.float32),
            pltpu.VMEM((2, rows, 128), jnp.float32),
            pltpu.VMEM((BLK, BLK), jnp.bfloat16),
        ],
        compiler_params=pltpu.CompilerParams(vmem_limit_bytes=40 * 1024 * 1024),
        cost_estimate=pl.CostEstimate(
            flops=40_000_000_000, bytes_accessed=8_000_000, transcendentals=100_000_000
        ),
        name="stick",
    )(count, q_aug, kv)


def augment_q(q, offs):
    R = q.shape[0]
    q4 = q.reshape(R, 2, 4, HD).transpose(1, 2, 0, 3).reshape(2, 4 * R, HD)
    rest = offs * 8.0
    terms = []
    for _ in range(3):
        term = rest.astype(jnp.bfloat16)
        terms.append(term)
        rest = rest - term.astype(jnp.float32)
    terms = jnp.stack(terms, 1).reshape(2, 4, 3)
    terms = jnp.broadcast_to(terms[:, :, None, :], (2, 4, R, 3)).reshape(2, 4 * R, 3)
    zeros = jnp.zeros((4 * R, HD), jnp.bfloat16)
    one = jnp.ones((4 * R, 1), jnp.bfloat16)
    none = jnp.zeros((4 * R, 1), jnp.bfloat16)
    tail = jnp.zeros((4 * R, 123), jnp.bfloat16)
    return jnp.stack(
        [
            jnp.concatenate([q4[0], zeros, one, none, terms[0], tail], 1),
            jnp.concatenate([zeros, q4[1], none, one, terms[1], tail], 1),
        ]
    )


def augment_kv(k, v, b):
    R = k.shape[0]
    return jnp.concatenate(
        [k, b * 8, jnp.ones((R, 3), jnp.bfloat16), jnp.zeros((R, 123), jnp.bfloat16), v], 1
    )


def body(
    query_rows,
    key_rows,
    value_rows,
    key_bias,
    head_offset,
    out_weight,
    expert_input,
    expert_gain,
    routes,
    route_weight,
    gate_weight,
    up_weight,
    down_weight,
):
    block_rows = query_rows.shape[0]
    all_kv = lax.all_gather(
        augment_kv(key_rows, value_rows, key_bias), "ep", axis=0, tiled=True
    )
    count = (lax.axis_index("ep") + 1).astype(jnp.int32).reshape(1)
    stacked = attention(count, augment_q(query_rows, head_offset), all_kv)
    heads_out = (
        stacked.reshape(8, block_rows, HD).transpose(1, 0, 2).reshape(block_rows, 8 * HD)
    )
    mixed_a = lax.psum_scatter(
        jnp.dot(heads_out, out_weight, preferred_element_type=jnp.float32).astype(jnp.bfloat16),
        "tp",
        scatter_dimension=0,
        tiled=True,
    )
    normed = rms_normed(expert_input, expert_gain)
    tok_count = normed.shape[0]
    top_count = routes.shape[1]
    model_width = normed.shape[1]
    expert_count = lax.axis_size("ep")
    capacity = max(2, 3 * tok_count * top_count // (2 * expert_count))
    flat_route = routes.reshape(-1)
    one_hot = (flat_route[:, None] == jnp.arange(expert_count)[None, :]).astype(jnp.int32)
    before = jnp.cumsum(one_hot, axis=0) - one_hot
    slot_index = (flat_route * capacity + jnp.sum(before * one_hot, axis=1)).reshape(
        tok_count, top_count
    )
    slot_ids = jnp.arange(expert_count * capacity)
    dispatch = jnp.sum(
        (slot_index[None, :, :] == slot_ids[:, None, None]).astype(jnp.int32), axis=2
    ).astype(jnp.bfloat16)
    outgoing = (
        jnp.dot(dispatch, normed, preferred_element_type=jnp.float32)
        .astype(jnp.bfloat16)
        .reshape(expert_count, capacity, model_width)
    )
    source_rows = expert_count * capacity
    arrived = lax.all_to_all(outgoing, "ep", split_axis=0, concat_axis=0, tiled=True)
    row_piece = lax.all_gather(arrived.reshape(source_rows, model_width), "tp", axis=0, tiled=True)
    gate_act = jnp.dot(row_piece, gate_weight[0], preferred_element_type=jnp.float32)
    up_act = jnp.dot(row_piece, up_weight[0], preferred_element_type=jnp.float32)
    hidden_all = (jax.nn.silu(gate_act) * up_act).astype(jnp.bfloat16)
    expert_result = lax.psum_scatter(
        jnp.dot(hidden_all, down_weight[0], preferred_element_type=jnp.float32).astype(
            jnp.bfloat16
        ),
        "tp",
        scatter_dimension=0,
        tiled=True,
    )
    returned = lax.all_to_all(
        expert_result.reshape(expert_count, capacity, model_width),
        "ep",
        split_axis=0,
        concat_axis=0,
        tiled=True,
    )
    picked_rows = returned.reshape(-1, model_width)[slot_index.reshape(-1)].reshape(
        tok_count, top_count, model_width
    )
    mixed_b = jnp.sum(picked_rows.astype(jnp.float32) * route_weight[:, :, None], axis=1).astype(
        jnp.bfloat16
    )
    return (mixed_a, mixed_b)


def solution(mesh):
    return jax.shard_map(
        body,
        mesh=mesh,
        in_specs=(
            P("ep", "tp"),
            P("ep", "tp"),
            P("ep", "tp"),
            P("ep", "tp"),
            P("tp"),
            P("tp", None),
            P(("ep", "tp"), None),
            P(),
            P(("ep", "tp"), None),
            P(("ep", "tp"), None),
            P("ep", None, "tp"),
            P("ep", None, "tp"),
            P("ep", "tp", None),
        ),
        out_specs=(P(("ep", "tp"), None), P(("ep", "tp"), None)),
        check_vma=False,
    )
```

```python
import functools
import math

import jax
import jax.numpy as jnp
from jax import lax
from jax.experimental import pallas as pl
from jax.experimental.pallas import tpu as pltpu
from jax.sharding import PartitionSpec as P

HD = 64
BLK = 256
EPSILON = 1e-06
TO_LOG2 = math.log2(math.e) / math.sqrt(HD)


def rms_normed(rows, gain):
    values = rows.astype(jnp.float32)
    scaled = values * lax.rsqrt(jnp.mean(values * values, axis=-1, keepdims=True) + EPSILON)
    return (scaled * gain).astype(jnp.bfloat16)


def stick_kernel(count_ref, q_ref, kv_ref, o_ref, acc, surv, tri, *, tile):
    count = count_ref[0]
    rows = q_ref.shape[1]
    at_row = lax.broadcasted_iota(jnp.int32, (BLK, BLK), 0)
    at_col = lax.broadcasted_iota(jnp.int32, (BLK, BLK), 1)
    tri[...] = jnp.where(at_row > at_col, -1.0, 0.0).astype(jnp.bfloat16)
    acc[...] = jnp.zeros_like(acc)
    surv[...] = jnp.zeros_like(surv)

    def block(index, diagonal):
        at = pl.multiple_of(index * BLK, BLK)
        keys = kv_ref[pl.ds(at, BLK), 0:256]
        for g in range(2):
            vals = kv_ref[pl.ds(at, BLK), 256 + HD * g : 256 + HD * (g + 1)]
            for m in range(rows // tile):
                part = slice(m * tile, (m + 1) * tile)
                z = (
                    lax.dot_general(
                        q_ref[g, part, :],
                        keys,
                        (((1,), (1,)), ((), ())),
                        preferred_element_type=jnp.float32,
                    )
                    * TO_LOG2
                )
                if diagonal:
                    query = lax.broadcasted_iota(jnp.int32, (tile, BLK), 0) % BLK
                    key = lax.broadcasted_iota(jnp.int32, (tile, BLK), 1)
                    z = jnp.where(key < query, z, -1e30)
                leave = jnp.maximum(z, jnp.log2(1.0 + jnp.exp2(jnp.minimum(z, 100.0))))
                after = (
                    jnp.dot(
                        leave.astype(jnp.bfloat16), tri[...], preferred_element_type=jnp.float32
                    )
                    - leave
                )
                s = surv[g, part, :]
                w = jnp.exp2(z + after + jnp.concatenate([s, s], axis=1)).astype(jnp.bfloat16)
                acc[g, part, :] += jnp.dot(w, vals, preferred_element_type=jnp.float32)
                surv[g, part, :] = s + jnp.broadcast_to(after[:, 0:1], s.shape)

    block(count - 1, True)

    def step(i, _):
        block(count - 2 - i, False)
        return 0

    lax.fori_loop(0, count - 1, step, 0)
    o_ref[...] = acc[...].astype(jnp.bfloat16)


def attention(count, q_aug, kv, tile=512):
    rows = q_aug.shape[1]
    return pl.pallas_call(
        functools.partial(stick_kernel, tile=tile),
        out_shape=jax.ShapeDtypeStruct((2, rows, HD), jnp.bfloat16),
        in_specs=[
            pl.BlockSpec(memory_space=pltpu.SMEM),
            pl.BlockSpec(memory_space=pltpu.VMEM),
            pl.BlockSpec(memory_space=pltpu.VMEM),
        ],
        out_specs=pl.BlockSpec(memory_space=pltpu.VMEM),
        scratch_shapes=[
            pltpu.VMEM((2, rows, HD), jnp.float32),
            pltpu.VMEM((2, rows, 128), jnp.float32),
            pltpu.VMEM((BLK, BLK), jnp.bfloat16),
        ],
        compiler_params=pltpu.CompilerParams(vmem_limit_bytes=40 * 1024 * 1024),
        cost_estimate=pl.CostEstimate(
            flops=40_000_000_000, bytes_accessed=8_000_000, transcendentals=100_000_000
        ),
        name="stick",
    )(count, q_aug, kv)


def augment_q(q, offs):
    R = q.shape[0]
    q4 = q.reshape(R, 2, 4, HD).transpose(1, 2, 0, 3).reshape(2, 4 * R, HD)
    rest = offs * 8.0
    terms = []
    for _ in range(3):
        term = rest.astype(jnp.bfloat16)
        terms.append(term)
        rest = rest - term.astype(jnp.float32)
    terms = jnp.stack(terms, 1).reshape(2, 4, 3)
    terms = jnp.broadcast_to(terms[:, :, None, :], (2, 4, R, 3)).reshape(2, 4 * R, 3)
    zeros = jnp.zeros((4 * R, HD), jnp.bfloat16)
    one = jnp.ones((4 * R, 1), jnp.bfloat16)
    none = jnp.zeros((4 * R, 1), jnp.bfloat16)
    tail = jnp.zeros((4 * R, 123), jnp.bfloat16)
    return jnp.stack(
        [
            jnp.concatenate([q4[0], zeros, one, none, terms[0], tail], 1),
            jnp.concatenate([zeros, q4[1], none, one, terms[1], tail], 1),
        ]
    )


def augment_kv(k, v, b):
    R = k.shape[0]
    return jnp.concatenate(
        [k, b * 8, jnp.ones((R, 3), jnp.bfloat16), jnp.zeros((R, 123), jnp.bfloat16), v], 1
    )


OFFSETS = (0, 1, 3, 2)
MESH = pl.DeviceIdType.MESH


def arrived(ref, sem):
    pltpu.make_async_copy(ref, ref, sem).wait()


def moe_kernel(
    out_ref,
    wg_any,
    wu_any,
    wd_any,
    ret_ref,
    wg,
    wu,
    wd,
    o4,
    rx,
    ys,
    first,
    mid,
    fin,
    res,
    r4,
    xs,
    hs,
    w_sem,
    a2a_send,
    a2a_recv,
    ag_send,
    ag_recv,
    fw_send,
    fw_recv,
    r1_send,
    r1_recv,
    rd_send,
    rm_send,
    fin_recv,
    ret_send,
    ret_recv,
):
    me = lax.axis_index("ep")
    x = lax.axis_index("tp")
    plane = me // 8
    place = lax.rem(me, 8)
    right = lax.rem(x + 1, 4)
    left = lax.rem(x + 3, 4)

    loads = [
        pltpu.make_async_copy(src.at[0], dst, w_sem.at[i])
        for i, (src, dst) in enumerate(((wg_any, wg), (wu_any, wu), (wd_any, wd)))
    ]
    for load in loads:
        load.start()

    barrier = pltpu.get_barrier_semaphore()

    def greet(i, _):
        pl.semaphore_signal(
            barrier, inc=1, device_id={"ep": lax.rem(me + i, 32)}, device_id_type=MESH
        )
        return 0

    lax.fori_loop(1, 32, greet, 0)
    for side in (left, right):
        pl.semaphore_signal(barrier, inc=1, device_id={"tp": side}, device_id_type=MESH)

    def repack(i, _):
        o4[pl.ds(i * 8, 8)] = out_ref[pl.ds(pl.multiple_of(i * 32, 32), 32), :].reshape(8, 4, 2048)
        return 0

    lax.fori_loop(0, 12, repack, 0)
    rx[0, pl.ds(place * 3, 3)] = o4[pl.ds(me * 3, 3)]
    pl.semaphore_wait(barrier, 33)

    def remote(src, dst, send, recv, device):
        copy = pltpu.make_async_remote_copy(
            src_ref=src,
            dst_ref=dst,
            send_sem=send,
            recv_sem=recv,
            device_id=device,
            device_id_type=MESH,
        )
        copy.start()

    for k, off in enumerate(OFFSETS):
        far = lax.rem(plane + off, 4) * 8

        def send_rows(i, _, k=k, far=far):
            j = lax.rem(place + i, 8)
            remote(
                o4.at[pl.ds((far + j) * 3, 3)],
                rx.at[k, pl.ds(place * 3, 3)],
                a2a_send,
                a2a_recv.at[k],
                {"ep": far + j},
            )
            return 0

        lax.fori_loop(1 if k == 0 else 0, 8, send_rows, 0)

    def gather_start(k):
        if k == 0:
            arrived(rx.at[0, pl.ds(0, 21)], a2a_recv.at[0])
        else:
            arrived(rx.at[k, pl.ds(0, 24)], a2a_recv.at[k])
        own = rx.at[k, pl.ds(0, 24)]
        remote(own, rx.at[k, pl.ds(24, 24)], ag_send.at[k, 0], ag_recv.at[k, 0], {"tp": right})
        remote(own, rx.at[k, pl.ds(48, 24)], ag_send.at[k, 1], ag_recv.at[k, 1], {"tp": left})

    def gather_forward(k):
        arrived(rx.at[k, pl.ds(24, 24)], ag_recv.at[k, 0])
        remote(
            rx.at[k, pl.ds(24, 12)],
            rx.at[k, pl.ds(72, 12)],
            fw_send.at[k, 0],
            fw_recv.at[k, 0],
            {"tp": right},
        )
        arrived(rx.at[k, pl.ds(48, 24)], ag_recv.at[k, 1])
        remote(
            rx.at[k, pl.ds(60, 12)],
            rx.at[k, pl.ds(84, 12)],
            fw_send.at[k, 1],
            fw_recv.at[k, 1],
            {"tp": left},
        )

    def expert(k):
        if k == 0:
            for load in loads:
                load.wait()
        arrived(rx.at[k, pl.ds(72, 12)], fw_recv.at[k, 0])
        arrived(rx.at[k, pl.ds(84, 12)], fw_recv.at[k, 1])

        def unpack(i, _):
            xs[pl.ds(pl.multiple_of(i * 32, 32), 32), :] = rx[k, pl.ds(i * 8, 8)].reshape(32, 2048)
            return 0

        lax.fori_loop(0, 12, unpack, 0)

        def hidden(at, width):
            rows = xs[...]
            gate = jnp.dot(rows, wg[:, pl.ds(at, width)], preferred_element_type=jnp.float32)
            up = jnp.dot(rows, wu[:, pl.ds(at, width)], preferred_element_type=jnp.float32)
            hs[:, pl.ds(at, width)] = (gate / (1.0 + jnp.exp(-gate)) * up).astype(jnp.bfloat16)

        def hidden_tile(i, _):
            hidden(pl.multiple_of(i * 256, 256), 256)
            return 0

        lax.fori_loop(0, 3, hidden_tile, 0)
        hidden(768, 128)

        def down(i, _):
            at = pl.multiple_of(i * 256, 256)
            part = jnp.dot(hs[...], wd[:, pl.ds(at, 256)], preferred_element_type=jnp.float32)
            ys[k, :, :, pl.ds(at, 256)] = part.astype(jnp.bfloat16).reshape(96, 4, 256)
            return 0

        lax.fori_loop(0, 8, down, 0)
        remote(
            ys.at[k, pl.ds(72, 12)],
            first.at[k, 0],
            r1_send.at[k, 0],
            r1_recv.at[k, 0],
            {"tp": right},
        )
        remote(
            ys.at[k, pl.ds(84, 12)],
            first.at[k, 1],
            r1_send.at[k, 1],
            r1_recv.at[k, 1],
            {"tp": left},
        )
        remote(
            ys.at[k, pl.ds(60, 12)],
            fin.at[k, 0, pl.ds(12, 12)],
            rd_send.at[k, 0],
            fin_recv.at[k, 0],
            {"tp": right},
        )
        remote(
            ys.at[k, pl.ds(24, 12)],
            fin.at[k, 1, pl.ds(0, 12)],
            rd_send.at[k, 1],
            fin_recv.at[k, 1],
            {"tp": left},
        )

    def added(k):
        for side, at, device in ((0, 48, right), (1, 36, left)):
            arrived(first.at[k, side], r1_recv.at[k, side])

            def add(i, _, side=side, at=at):
                both = ys[k, pl.ds(at + i, 1)].astype(jnp.float32) + first[
                    k, side, pl.ds(i, 1)
                ].astype(jnp.float32)
                mid[k, side, pl.ds(i, 1)] = both.astype(jnp.bfloat16)
                return 0

            lax.fori_loop(0, 12, add, 0)
            remote(
                mid.at[k, side],
                fin.at[k, side, pl.ds(12 * side, 12)],
                rm_send.at[k, side],
                fin_recv.at[k, 2 + side],
                {"tp": device},
            )

    def back(k):
        arrived(fin.at[k, 0, pl.ds(12, 12)], fin_recv.at[k, 0])
        arrived(fin.at[k, 1, pl.ds(0, 12)], fin_recv.at[k, 1])
        arrived(fin.at[k, 0, pl.ds(0, 12)], fin_recv.at[k, 2])
        arrived(fin.at[k, 1, pl.ds(12, 12)], fin_recv.at[k, 3])

        def add(i, _):
            total = ys[k, pl.ds(i, 1)].astype(jnp.float32)
            total = total + fin[k, 0, pl.ds(i, 1)].astype(jnp.float32)
            total = total + fin[k, 1, pl.ds(i, 1)].astype(jnp.float32)
            res[k, pl.ds(i, 1)] = total.astype(jnp.bfloat16)
            return 0

        lax.fori_loop(0, 24, add, 0)
        far = lax.rem(plane + 4 - OFFSETS[k], 4) * 8

        def send_back(i, _):
            j = lax.rem(place + i, 8)
            remote(
                res.at[k, pl.ds(j * 3, 3)],
                r4.at[pl.ds(me * 3, 3)],
                ret_send,
                ret_recv,
                {"ep": far + j},
            )
            return 0

        lax.fori_loop(1 if k == 0 else 0, 8, send_back, 0)
        if k == 0:
            r4[pl.ds(me * 3, 3)] = res[0, pl.ds(place * 3, 3)]

    gather_start(0)
    gather_start(1)
    gather_forward(0)
    gather_start(2)
    gather_forward(1)
    expert(0)
    gather_start(3)
    gather_forward(2)
    expert(1)
    added(0)
    gather_forward(3)
    expert(2)
    added(1)
    back(0)
    expert(3)
    added(2)
    back(1)
    added(3)
    back(2)
    back(3)

    arrived(o4.at[pl.ds(0, 93)], a2a_send)
    for k in range(4):
        for side in range(2):
            arrived(rx.at[k, pl.ds(0, 24)], ag_send.at[k, side])
            arrived(rx.at[k, pl.ds(24, 12)], fw_send.at[k, side])
            arrived(first.at[k, side], r1_send.at[k, side])
            arrived(first.at[k, side], rd_send.at[k, side])
            arrived(first.at[k, side], rm_send.at[k, side])
    arrived(o4.at[pl.ds(0, 93)], ret_send)
    arrived(r4.at[pl.ds(0, 93)], ret_recv)

    def unpack_back(i, _):
        ret_ref[pl.ds(pl.multiple_of(i * 32, 32), 32), :] = r4[pl.ds(i * 8, 8)].reshape(32, 2048)
        return 0

    lax.fori_loop(0, 12, unpack_back, 0)


def experts(outgoing, gate_weight, up_weight, down_weight):
    rows, width = outgoing.shape
    ff = gate_weight.shape[2]
    bf16 = jnp.bfloat16
    dma = pltpu.SemaphoreType.DMA
    return pl.pallas_call(
        moe_kernel,
        out_shape=jax.ShapeDtypeStruct((rows, width), bf16),
        in_specs=[pl.BlockSpec(memory_space=pltpu.VMEM)]
        + [pl.BlockSpec(memory_space=pl.ANY)] * 3,
        out_specs=pl.BlockSpec(memory_space=pltpu.VMEM),
        scratch_shapes=[
            pltpu.VMEM((width, ff), bf16),
            pltpu.VMEM((width, ff), bf16),
            pltpu.VMEM((ff, width), bf16),
            pltpu.VMEM((96, 4, width), bf16),
            pltpu.VMEM((4, 96, 4, width), bf16),
            pltpu.VMEM((4, 96, 4, width), bf16),
            pltpu.VMEM((4, 2, 12, 4, width), bf16),
            pltpu.VMEM((4, 2, 12, 4, width), bf16),
            pltpu.VMEM((4, 2, 24, 4, width), bf16),
            pltpu.VMEM((4, 24, 4, width), bf16),
            pltpu.VMEM((96, 4, width), bf16),
            pltpu.VMEM((rows, width), bf16),
            pltpu.VMEM((rows, ff), bf16),
            dma((3,)),
            dma,
            dma((4,)),
            dma((4, 2)),
            dma((4, 2)),
            dma((4, 2)),
            dma((4, 2)),
            dma((4, 2)),
            dma((4, 2)),
            dma((4, 2)),
            dma((4, 2)),
            dma((4, 4)),
            dma,
            dma,
        ],
        compiler_params=pltpu.CompilerParams(
            vmem_limit_bytes=60 * 1024 * 1024, collective_id=0, has_side_effects=True
        ),
        cost_estimate=pl.CostEstimate(
            flops=17_000_000_000, bytes_accessed=14_000_000, transcendentals=1_400_000
        ),
        name="experts",
    )(outgoing, gate_weight, up_weight, down_weight)


def body(
    query_rows,
    key_rows,
    value_rows,
    key_bias,
    head_offset,
    out_weight,
    expert_input,
    expert_gain,
    routes,
    route_weight,
    gate_weight,
    up_weight,
    down_weight,
):
    block_rows = query_rows.shape[0]
    all_kv = lax.all_gather(
        augment_kv(key_rows, value_rows, key_bias), "ep", axis=0, tiled=True
    )
    count = (lax.axis_index("ep") + 1).astype(jnp.int32).reshape(1)
    stacked = attention(count, augment_q(query_rows, head_offset), all_kv)
    heads_out = (
        stacked.reshape(8, block_rows, HD).transpose(1, 0, 2).reshape(block_rows, 8 * HD)
    )
    mixed_a = lax.psum_scatter(
        jnp.dot(heads_out, out_weight, preferred_element_type=jnp.float32).astype(jnp.bfloat16),
        "tp",
        scatter_dimension=0,
        tiled=True,
    )
    normed = rms_normed(expert_input, expert_gain)
    tok_count = normed.shape[0]
    top_count = routes.shape[1]
    model_width = normed.shape[1]
    expert_count = lax.axis_size("ep")
    capacity = max(2, 3 * tok_count * top_count // (2 * expert_count))
    flat_route = routes.reshape(-1)
    one_hot = (flat_route[:, None] == jnp.arange(expert_count)[None, :]).astype(jnp.int32)
    before = jnp.cumsum(one_hot, axis=0) - one_hot
    slot_index = (flat_route * capacity + jnp.sum(before * one_hot, axis=1)).reshape(
        tok_count, top_count
    )
    slot_ids = jnp.arange(expert_count * capacity)
    dispatch = jnp.sum(
        (slot_index[None, :, :] == slot_ids[:, None, None]).astype(jnp.int32), axis=2
    ).astype(jnp.bfloat16)
    outgoing = (
        jnp.dot(dispatch, normed, preferred_element_type=jnp.float32)
        .astype(jnp.bfloat16)
    )
    returned = experts(outgoing, gate_weight, up_weight, down_weight)
    picked_rows = returned.reshape(-1, model_width)[slot_index.reshape(-1)].reshape(
        tok_count, top_count, model_width
    )
    mixed_b = jnp.sum(picked_rows.astype(jnp.float32) * route_weight[:, :, None], axis=1).astype(
        jnp.bfloat16
    )
    return (mixed_a, mixed_b)


def solution(mesh):
    return jax.shard_map(
        body,
        mesh=mesh,
        in_specs=(
            P("ep", "tp"),
            P("ep", "tp"),
            P("ep", "tp"),
            P("ep", "tp"),
            P("tp"),
            P("tp", None),
            P(("ep", "tp"), None),
            P(),
            P(("ep", "tp"), None),
            P(("ep", "tp"), None),
            P("ep", None, "tp"),
            P("ep", None, "tp"),
            P("ep", "tp", None),
        ),
        out_specs=(P(("ep", "tp"), None), P(("ep", "tp"), None)),
        check_vma=False,
    )
```

```python
import math

import jax
import jax.numpy as jnp
from jax import lax
from jax.experimental import pallas as pl
from jax.experimental.pallas import tpu as pltpu
from jax.sharding import PartitionSpec as P

HD = 64
BLK = 256
CAP = 12
EPSILON = 1e-06
TO_LOG2 = math.log2(math.e) / math.sqrt(HD)
OFFSETS = (0, 1, 3, 2)
SEGMENTS = 8
TILE = 512
MESH = pl.DeviceIdType.MESH


def arrived(ref, sem):
    pltpu.make_async_copy(ref, ref, sem).wait()


def remote(src, dst, send, recv, device):
    pltpu.make_async_remote_copy(
        src_ref=src,
        dst_ref=dst,
        send_sem=send,
        recv_sem=recv,
        device_id=device,
        device_id_type=MESH,
    ).start()


def iota(shape, dim):
    return lax.broadcasted_iota(jnp.int32, shape, dim)


def step_kernel(
    query_ref,
    key_ref,
    value_ref,
    bias_ref,
    offset_ref,
    x_ref,
    gain_ref,
    routes_ref,
    rw_ref,
    ow_any,
    wg_any,
    wu_any,
    wd_any,
    mixed_a_ref,
    mixed_b_ref,
    ow,
    wg,
    wu,
    wd,
    o4,
    rx,
    ys,
    first,
    mid,
    fin,
    res,
    r4,
    xs,
    hs,
    kt,
    vv,
    qa,
    acc,
    surv,
    tri,
    ho,
    po,
    pm,
    w_sem,
    a2a_send,
    a2a_recv,
    ag_send,
    ag_recv,
    fw_send,
    fw_recv,
    r1_send,
    r1_recv,
    rd_send,
    rm_send,
    fin_recv,
    ret_send,
    ret_recv,
    ky_send,
    ky_recv,
    kz_send,
    kz_recv,
    kc_send,
    kc_recv,
    po_send,
    po_recv,
):
    me = lax.axis_index("ep")
    x = lax.axis_index("tp")
    plane = me // 8
    place = lax.rem(me, 8)
    row = place // 2
    core = lax.rem(place, 2)
    right = lax.rem(x + 1, 4)
    left = lax.rem(x + 3, 4)
    across = lax.rem(x + 2, 4)
    bf16, f32 = jnp.bfloat16, jnp.float32

    loads = [
        pltpu.make_async_copy(src, dst, w_sem.at[i])
        for i, (src, dst) in enumerate(
            ((wg_any.at[0], wg), (wu_any.at[0], wu), (wd_any.at[0], wd), (ow_any, ow))
        )
    ]
    for load in loads:
        load.start()

    barrier = pltpu.get_barrier_semaphore()

    def greet(i, _):
        pl.semaphore_signal(
            barrier, inc=1, device_id={"ep": lax.rem(me + i, 32)}, device_id_type=MESH
        )
        return 0

    lax.fori_loop(1, 32, greet, 0)
    for side in (left, right, across):
        pl.semaphore_signal(barrier, inc=1, device_id={"tp": side}, device_id_type=MESH)

    def clear(i, _):
        kt[i, pl.ds(144, 112), :] = jnp.zeros((112, BLK), bf16)
        return 0

    lax.fori_loop(0, 32, clear, 0)
    own = plane * 8 + core * 4 + row
    kt[own, pl.ds(0, 128), :] = key_ref[...].astype(f32).T.astype(bf16)
    bias = bias_ref[...].astype(f32) * 8.0
    sub = iota((16, BLK), 0)
    extra = jnp.where(sub == 0, bias[0:1, :], jnp.where(sub == 1, bias[1:2, :], 0.0))
    extra = jnp.where((sub >= 2) & (sub <= 4), 1.0, extra)
    kt[own, pl.ds(128, 16), :] = extra.astype(bf16)
    vv[own, :, pl.ds(0, 128)] = value_ref[pl.ds(0, 128), :]
    vv[own, :, pl.ds(128, 128)] = value_ref[pl.ds(128, 128), :]

    expert_at = iota((32, 128), 0)
    earlier = jnp.where(iota((128, 128), 0) < iota((128, 128), 1), 1.0, 0.0).astype(bf16)
    base = (expert_at * CAP).astype(f32)
    slots = []
    for c in range(2):
        named = expert_at == routes_ref[c : c + 1, :]
        count = jnp.where(named, 1.0, 0.0)
        rank = base + jnp.dot(count.astype(bf16), earlier, preferred_element_type=f32)
        slots.append(jnp.sum(jnp.where(named, rank, 0.0), axis=0, keepdims=True).astype(jnp.int32))
        base = base + jnp.sum(count, axis=1, keepdims=True)
    slot_at = iota((32 * CAP, 128), 0)

    def norm(i, _):
        at = pl.ds(pl.multiple_of(i * 32, 32), 32)
        values = x_ref[at, :].astype(f32)
        scale = lax.rsqrt(jnp.mean(values * values, axis=1, keepdims=True) + EPSILON)
        xs[at, :] = (values * scale * gain_ref[...]).astype(bf16)
        return 0

    lax.fori_loop(0, 4, norm, 0)
    pick = jnp.where((slot_at == slots[0]) | (slot_at == slots[1]), 1.0, 0.0).astype(bf16)

    def dispatch(i, _):
        at = pl.ds(pl.multiple_of(i * 256, 256), 256)
        rows = jnp.dot(pick, xs[pl.ds(0, 128), at], preferred_element_type=f32)
        o4[:, :, at] = rows.astype(bf16).reshape(96, 4, 256)
        return 0

    lax.fori_loop(0, 8, dispatch, 0)
    rx[0, pl.ds(place * 3, 3)] = o4[pl.ds(me * 3, 3)]
    pl.semaphore_wait(barrier, 34)

    def along_y(d):
        return {"ep": plane * 8 + lax.rem(row + d, 4) * 2 + core}

    def along_z(d):
        return {"ep": lax.rem(plane + d, 4) * 8 + place}

    def kt_y(d):
        return kt.at[plane * 8 + core * 4 + lax.rem(row + d, 4), pl.ds(0, 144)]

    def vv_y(d):
        return vv.at[plane * 8 + core * 4 + lax.rem(row + d, 4)]

    def kt_z(d, c=core):
        return kt.at[pl.ds(lax.rem(plane + d, 4) * 8 + c * 4, 4), pl.ds(0, 144)]

    def vv_z(d, c=core):
        return vv.at[pl.ds(lax.rem(plane + d, 4) * 8 + c * 4, 4)]

    def keys_y():
        for s, d in enumerate((1, 3)):
            remote(kt_y(0), kt_y(0), ky_send.at[s, 0], ky_recv.at[s, 0], along_y(d))
            remote(vv_y(0), vv_y(0), ky_send.at[s, 1], ky_recv.at[s, 1], along_y(d))

    def keys_y_on():
        arrived(kt_y(3), ky_recv.at[0, 0])
        remote(kt_y(3), kt_y(3), ky_send.at[2, 0], ky_recv.at[2, 0], along_y(1))
        arrived(vv_y(1), ky_recv.at[1, 1])
        remote(vv_y(1), vv_y(1), ky_send.at[2, 1], ky_recv.at[2, 1], along_y(3))
        arrived(vv_y(3), ky_recv.at[0, 1])
        arrived(kt_y(1), ky_recv.at[1, 0])

    def keys_z():
        arrived(kt_y(2), ky_recv.at[2, 0])
        arrived(vv_y(2), ky_recv.at[2, 1])
        for s, d in enumerate((1, 3)):
            remote(kt_z(0), kt_z(0), kz_send.at[s, 0], kz_recv.at[s, 0], along_z(d))
            remote(vv_z(0), vv_z(0), kz_send.at[s, 1], kz_recv.at[s, 1], along_z(d))

    def keys_z_on():
        arrived(kt_z(3), kz_recv.at[0, 0])
        remote(kt_z(3), kt_z(3), kz_send.at[2, 0], kz_recv.at[2, 0], along_z(1))
        arrived(vv_z(1), kz_recv.at[1, 1])
        remote(vv_z(1), vv_z(1), kz_send.at[2, 1], kz_recv.at[2, 1], along_z(3))
        arrived(vv_z(3), kz_recv.at[0, 1])
        arrived(kt_z(1), kz_recv.at[1, 0])

    def keys_core():
        arrived(kt_z(2), kz_recv.at[2, 0])
        arrived(vv_z(2), kz_recv.at[2, 1])
        for d in range(4):
            device = {"ep": me + 1 - 2 * core}
            remote(kt_z(d), kt_z(d), kc_send.at[d, 0], kc_recv.at[d, 0], device)
            remote(vv_z(d), vv_z(d), kc_send.at[d, 1], kc_recv.at[d, 1], device)

    def keys_here():
        for d in range(4):
            arrived(kt_z(d, 1 - core), kc_recv.at[d, 0])
            arrived(vv_z(d, 1 - core), kc_recv.at[d, 1])

    keys_y()

    for k, off in enumerate(OFFSETS):
        far = lax.rem(plane + off, 4) * 8

        def send_rows(i, _, k=k, far=far):
            j = lax.rem(place + i, 8)
            remote(
                o4.at[pl.ds((far + j) * 3, 3)],
                rx.at[k, pl.ds(place * 3, 3)],
                a2a_send,
                a2a_recv.at[k],
                {"ep": far + j},
            )
            return 0

        lax.fori_loop(1 if k == 0 else 0, 8, send_rows, 0)

    def gather_start(k):
        if k == 0:
            arrived(rx.at[0, pl.ds(0, 21)], a2a_recv.at[0])
        else:
            arrived(rx.at[k, pl.ds(0, 24)], a2a_recv.at[k])
        own = rx.at[k, pl.ds(0, 24)]
        remote(own, rx.at[k, pl.ds(24, 24)], ag_send.at[k, 0], ag_recv.at[k, 0], {"tp": right})
        remote(own, rx.at[k, pl.ds(48, 24)], ag_send.at[k, 1], ag_recv.at[k, 1], {"tp": left})

    def gather_forward(k):
        arrived(rx.at[k, pl.ds(24, 24)], ag_recv.at[k, 0])
        remote(
            rx.at[k, pl.ds(24, 12)],
            rx.at[k, pl.ds(72, 12)],
            fw_send.at[k, 0],
            fw_recv.at[k, 0],
            {"tp": right},
        )
        arrived(rx.at[k, pl.ds(48, 24)], ag_recv.at[k, 1])
        remote(
            rx.at[k, pl.ds(60, 12)],
            rx.at[k, pl.ds(84, 12)],
            fw_send.at[k, 1],
            fw_recv.at[k, 1],
            {"tp": left},
        )

    def expert(k):
        if k == 0:
            for load in loads[:3]:
                load.wait()
        arrived(rx.at[k, pl.ds(72, 12)], fw_recv.at[k, 0])
        arrived(rx.at[k, pl.ds(84, 12)], fw_recv.at[k, 1])

        def unpack(i, _):
            xs[pl.ds(pl.multiple_of(i * 32, 32), 32), :] = rx[k, pl.ds(i * 8, 8)].reshape(32, 2048)
            return 0

        lax.fori_loop(0, 12, unpack, 0)

        def hidden(at, width):
            rows = xs[...]
            gate = jnp.dot(rows, wg[:, pl.ds(at, width)], preferred_element_type=jnp.float32)
            up = jnp.dot(rows, wu[:, pl.ds(at, width)], preferred_element_type=jnp.float32)
            hs[:, pl.ds(at, width)] = (gate / (1.0 + jnp.exp(-gate)) * up).astype(jnp.bfloat16)

        def hidden_tile(i, _):
            hidden(pl.multiple_of(i * 256, 256), 256)
            return 0

        lax.fori_loop(0, 3, hidden_tile, 0)
        hidden(768, 128)

        def down(i, _):
            at = pl.multiple_of(i * 256, 256)
            part = jnp.dot(hs[...], wd[:, pl.ds(at, 256)], preferred_element_type=jnp.float32)
            ys[k, :, :, pl.ds(at, 256)] = part.astype(jnp.bfloat16).reshape(96, 4, 256)
            return 0

        lax.fori_loop(0, 8, down, 0)
        remote(
            ys.at[k, pl.ds(72, 12)],
            first.at[k, 0],
            r1_send.at[k, 0],
            r1_recv.at[k, 0],
            {"tp": right},
        )
        remote(
            ys.at[k, pl.ds(84, 12)],
            first.at[k, 1],
            r1_send.at[k, 1],
            r1_recv.at[k, 1],
            {"tp": left},
        )
        remote(
            ys.at[k, pl.ds(60, 12)],
            fin.at[k, 0, pl.ds(12, 12)],
            rd_send.at[k, 0],
            fin_recv.at[k, 0],
            {"tp": right},
        )
        remote(
            ys.at[k, pl.ds(24, 12)],
            fin.at[k, 1, pl.ds(0, 12)],
            rd_send.at[k, 1],
            fin_recv.at[k, 1],
            {"tp": left},
        )

    def added(k):
        for side, at, device in ((0, 48, right), (1, 36, left)):
            arrived(first.at[k, side], r1_recv.at[k, side])

            def add(i, _, side=side, at=at):
                both = ys[k, pl.ds(at + i, 1)].astype(jnp.float32) + first[
                    k, side, pl.ds(i, 1)
                ].astype(jnp.float32)
                mid[k, side, pl.ds(i, 1)] = both.astype(jnp.bfloat16)
                return 0

            lax.fori_loop(0, 12, add, 0)
            remote(
                mid.at[k, side],
                fin.at[k, side, pl.ds(12 * side, 12)],
                rm_send.at[k, side],
                fin_recv.at[k, 2 + side],
                {"tp": device},
            )

    def back(k):
        arrived(fin.at[k, 0, pl.ds(12, 12)], fin_recv.at[k, 0])
        arrived(fin.at[k, 1, pl.ds(0, 12)], fin_recv.at[k, 1])
        arrived(fin.at[k, 0, pl.ds(0, 12)], fin_recv.at[k, 2])
        arrived(fin.at[k, 1, pl.ds(12, 12)], fin_recv.at[k, 3])

        def add(i, _):
            total = ys[k, pl.ds(i, 1)].astype(jnp.float32)
            total = total + fin[k, 0, pl.ds(i, 1)].astype(jnp.float32)
            total = total + fin[k, 1, pl.ds(i, 1)].astype(jnp.float32)
            res[k, pl.ds(i, 1)] = total.astype(jnp.bfloat16)
            return 0

        lax.fori_loop(0, 24, add, 0)
        far = lax.rem(plane + 4 - OFFSETS[k], 4) * 8

        def send_back(i, _):
            j = lax.rem(place + i, 8)
            remote(
                res.at[k, pl.ds(j * 3, 3)],
                r4.at[pl.ds(me * 3, 3)],
                ret_send,
                ret_recv,
                {"ep": far + j},
            )
            return 0

        lax.fori_loop(1 if k == 0 else 0, 8, send_back, 0)
        if k == 0:
            r4[pl.ds(me * 3, 3)] = res[0, pl.ds(place * 3, 3)]

    def queries():
        lane = iota((1, 128), 1)
        half = iota((BLK, 128), 1) < HD
        for g in range(2):
            for j in range(4):
                h = 4 * g + j
                pair = query_ref[:, 128 * (h // 2) : 128 * (h // 2 + 1)].astype(f32)
                if h % 2 != g:
                    pair = pltpu.roll(pair, HD, 1)
                qa[g, pl.ds(BLK * j, BLK), pl.ds(0, 128)] = jnp.where(
                    half if g == 0 else ~half, pair, 0.0
                ).astype(bf16)
                rest = jnp.full((1, 128), offset_ref[h] * 8.0, f32)
                columns = jnp.where(lane == g, 1.0, 0.0)
                for t in range(3):
                    term = rest.astype(bf16).astype(f32)
                    columns = jnp.where(lane == 2 + t, term, columns)
                    rest = rest - term
                qa[g, pl.ds(BLK * j, BLK), pl.ds(128, 128)] = jnp.broadcast_to(
                    columns, (BLK, 128)
                ).astype(bf16)
        tri[...] = jnp.where(iota((BLK, BLK), 0) > iota((BLK, BLK), 1), -1.0, 0.0).astype(bf16)
        acc[...] = jnp.zeros_like(acc)
        surv[...] = jnp.zeros_like(surv)

    def block(index, diagonal):
        at = (index // 8) * 8 + lax.rem(index, 2) * 4 + lax.rem(index, 8) // 2
        keys = kt[at]
        for g in range(2):
            vals = jnp.concatenate(
                [
                    vv[at, :, HD * g : HD * (g + 1)],
                    vv[at, :, 128 + HD * g : 128 + HD * (g + 1)],
                ],
                axis=0,
            )
            for m in range(4 * BLK // TILE):
                part = slice(m * TILE, (m + 1) * TILE)
                z = jnp.dot(qa[g, part, :], keys, preferred_element_type=f32) * TO_LOG2
                if diagonal:
                    z = jnp.where(
                        iota((TILE, BLK), 1) < lax.rem(iota((TILE, BLK), 0), BLK), z, -1e30
                    )
                leave = jnp.maximum(z, jnp.log2(1.0 + jnp.exp2(jnp.minimum(z, 100.0))))
                after = jnp.dot(leave.astype(bf16), tri[...], preferred_element_type=f32) - leave
                s = surv[g, part, :]
                w = jnp.exp2(z + after + jnp.concatenate([s, s], axis=1)).astype(bf16)
                acc[g, part, :] += jnp.dot(w, vals, preferred_element_type=f32)
                surv[g, part, :] = s + jnp.broadcast_to(after[:, 0:1], s.shape)

    def attend(first_part, last_part):
        def step(i, _):
            block(me - 1 - i, False)
            return 0

        lax.fori_loop(me * first_part // SEGMENTS, me * last_part // SEGMENTS, step, 0)

    def project():
        for h in range(0, 8, 2):
            pair = [
                acc[(h + i) // 4, pl.ds(BLK * ((h + i) % 4), BLK), :].astype(bf16)
                for i in range(2)
            ]
            ho[:, pl.ds(HD * h, 2 * HD)] = jnp.concatenate(pair, axis=1)
        loads[3].wait()

        def out(i, _):
            at = pl.ds(pl.multiple_of(i * 256, 256), 256)
            part = jnp.dot(ho[...], ow[:, at], preferred_element_type=f32).astype(bf16)
            po[:, :, at] = part.reshape(4, 64, 256)
            return 0

        lax.fori_loop(0, 8, out, 0)
        for s, side in enumerate((across, right, left)):
            remote(po.at[side], pm.at[s], po_send.at[s], po_recv.at[s], {"tp": side})

    def mixed():
        for s in range(3):
            arrived(pm.at[s], po_recv.at[s])
        total = po[x].astype(f32)
        for s in range(3):
            total = total + pm[s].astype(f32)
        mixed_a_ref[...] = total.astype(bf16)

    gather_start(0)
    keys_y_on()
    gather_start(1)
    keys_z()
    gather_start(2)
    gather_forward(0)
    queries()
    keys_z_on()
    gather_start(3)
    gather_forward(1)
    keys_core()
    expert(0)
    gather_forward(2)
    expert(1)
    added(0)
    gather_forward(3)
    expert(2)
    added(1)
    back(0)
    expert(3)
    added(2)
    keys_here()
    block(me, True)
    attend(0, 1)
    added(3)
    back(1)
    attend(1, 3)
    back(2)
    attend(3, 5)
    back(3)
    attend(5, SEGMENTS)
    project()

    arrived(o4.at[pl.ds(0, 93)], a2a_send)
    for k in range(4):
        for side in range(2):
            arrived(rx.at[k, pl.ds(0, 24)], ag_send.at[k, side])
            arrived(rx.at[k, pl.ds(24, 12)], fw_send.at[k, side])
            arrived(first.at[k, side], r1_send.at[k, side])
            arrived(first.at[k, side], rd_send.at[k, side])
            arrived(first.at[k, side], rm_send.at[k, side])
    for s in range(3):
        arrived(kt_y(0), ky_send.at[s, 0])
        arrived(vv_y(0), ky_send.at[s, 1])
        arrived(kt_z(0), kz_send.at[s, 0])
        arrived(vv_z(0), kz_send.at[s, 1])
    for d in range(4):
        arrived(kt_z(0), kc_send.at[d, 0])
        arrived(vv_z(0), kc_send.at[d, 1])
    arrived(o4.at[pl.ds(0, 93)], ret_send)
    arrived(r4.at[pl.ds(0, 93)], ret_recv)

    def unpack_back(i, _):
        xs[pl.ds(pl.multiple_of(i * 32, 32), 32), :] = r4[pl.ds(i * 8, 8)].reshape(32, 2048)
        return 0

    lax.fori_loop(0, 12, unpack_back, 0)
    weight = jnp.where(slot_at == slots[0], rw_ref[0:1, :], 0.0)
    weight = weight + jnp.where(slot_at == slots[1], rw_ref[1:2, :], 0.0)
    high = weight.astype(bf16)
    low = (weight - high.astype(f32)).astype(bf16)

    def combine(i, _):
        at = pl.ds(pl.multiple_of(i * 256, 256), 256)
        rows = xs[:, at]
        dims = (((0,), (0,)), ((), ()))
        total = lax.dot_general(high, rows, dims, preferred_element_type=f32)
        total = total + lax.dot_general(low, rows, dims, preferred_element_type=f32)
        mixed_b_ref[:, at] = total.astype(bf16)
        return 0

    lax.fori_loop(0, 8, combine, 0)
    mixed()
    for s in range(3):
        arrived(pm.at[s], po_send.at[s])


def body(
    query_rows,
    key_rows,
    value_rows,
    key_bias,
    head_offset,
    out_weight,
    expert_input,
    expert_gain,
    routes,
    route_weight,
    gate_weight,
    up_weight,
    down_weight,
):
    width, ff = gate_weight.shape[1:]
    tokens = expert_input.shape[0]
    rows = 32 * CAP
    bf16, f32 = jnp.bfloat16, jnp.float32
    dma = pltpu.SemaphoreType.DMA
    vmem = pltpu.VMEM
    here, there = pl.BlockSpec(memory_space=vmem), pl.BlockSpec(memory_space=pl.ANY)
    return pl.pallas_call(
        step_kernel,
        out_shape=(
            jax.ShapeDtypeStruct((BLK // 4, width), bf16),
            jax.ShapeDtypeStruct((tokens, width), bf16),
        ),
        in_specs=[here] * 4
        + [pl.BlockSpec(memory_space=pltpu.SMEM)]
        + [here] * 4
        + [there] * 4,
        out_specs=(here, here),
        scratch_shapes=[
            vmem((8 * HD, width), bf16),
            vmem((width, ff), bf16),
            vmem((width, ff), bf16),
            vmem((ff, width), bf16),
            vmem((96, 4, width), bf16),
            vmem((4, 96, 4, width), bf16),
            vmem((4, 96, 4, width), bf16),
            vmem((4, 2, 12, 4, width), bf16),
            vmem((4, 2, 12, 4, width), bf16),
            vmem((4, 2, 24, 4, width), bf16),
            vmem((4, 24, 4, width), bf16),
            vmem((96, 4, width), bf16),
            vmem((rows, width), bf16),
            vmem((rows, ff), bf16),
            vmem((32, BLK, BLK), bf16),
            vmem((32, BLK // 2, BLK), bf16),
            vmem((2, 4 * BLK, 256), bf16),
            vmem((2, 4 * BLK, HD), f32),
            vmem((2, 4 * BLK, 128), f32),
            vmem((BLK, BLK), bf16),
            vmem((BLK, 8 * HD), bf16),
            vmem((4, BLK // 4, width), bf16),
            vmem((3, BLK // 4, width), bf16),
            dma((4,)),
            dma,
            dma((4,)),
            dma((4, 2)),
            dma((4, 2)),
            dma((4, 2)),
            dma((4, 2)),
            dma((4, 2)),
            dma((4, 2)),
            dma((4, 2)),
            dma((4, 2)),
            dma((4, 4)),
            dma,
            dma,
            dma((3, 2)),
            dma((3, 2)),
            dma((3, 2)),
            dma((3, 2)),
            dma((4, 2)),
            dma((4, 2)),
            dma((3,)),
            dma((3,)),
        ],
        compiler_params=pltpu.CompilerParams(
            vmem_limit_bytes=63 * 1024 * 1024, collective_id=0, has_side_effects=True
        ),
        name="step",
    )(
        query_rows,
        key_rows,
        value_rows,
        key_bias.T,
        head_offset,
        expert_input,
        expert_gain[None, :],
        routes.T,
        route_weight.T,
        out_weight,
        gate_weight,
        up_weight,
        down_weight,
    )


def solution(mesh):
    return jax.shard_map(
        body,
        mesh=mesh,
        in_specs=(
            P("ep", "tp"),
            P("ep", "tp"),
            P("ep", "tp"),
            P("ep", "tp"),
            P("tp"),
            P("tp", None),
            P(("ep", "tp"), None),
            P(),
            P(("ep", "tp"), None),
            P(("ep", "tp"), None),
            P("ep", None, "tp"),
            P("ep", None, "tp"),
            P("ep", "tp", None),
        ),
        out_specs=(P(("ep", "tp"), None), P(("ep", "tp"), None)),
        check_vma=False,
    )
```

```python
import math

import jax
import jax.numpy as jnp
from jax import lax
from jax.experimental import pallas as pl
from jax.experimental.pallas import tpu as pltpu
from jax.sharding import PartitionSpec as P

HD = 64
BLK = 256
CAP = 12
EPSILON = 1e-06
TO_LOG2 = math.log2(math.e) / math.sqrt(HD)
OFFSETS = (0, 1, 3, 2)
SHARE = 16
TILE = 512
MESH = pl.DeviceIdType.MESH


def arrived(ref, sem):
    pltpu.make_async_copy(ref, ref, sem).wait()


def remote(src, dst, send, recv, device):
    pltpu.make_async_remote_copy(
        src_ref=src,
        dst_ref=dst,
        send_sem=send,
        recv_sem=recv,
        device_id=device,
        device_id_type=MESH,
    ).start()


def iota(shape, dim):
    return lax.broadcasted_iota(jnp.int32, shape, dim)


def step_kernel(
    query_ref,
    key_ref,
    value_ref,
    bias_ref,
    offset_ref,
    x_ref,
    gain_ref,
    routes_ref,
    rw_ref,
    ow_any,
    wg_any,
    wu_any,
    wd_any,
    mixed_a_ref,
    mixed_b_ref,
    ow,
    wg,
    wu,
    wd,
    o4,
    rx,
    ys,
    first,
    mid,
    fin,
    res,
    r4,
    xs,
    hs,
    kt,
    vv,
    qa,
    acc,
    surv,
    tri,
    ho,
    po,
    pm,
    w_sem,
    a2a_send,
    a2a_recv,
    ag_send,
    ag_recv,
    fw_send,
    fw_recv,
    r1_send,
    r1_recv,
    rd_send,
    rm_send,
    fin_recv,
    ret_send,
    ret_recv,
    ky_send,
    ky_recv,
    kz_send,
    kz_recv,
    kc_send,
    kc_recv,
    po_send,
    po_recv,
    guest,
    far_out,
    far_in,
    pair_send,
    pair_recv,
):
    me = lax.axis_index("ep")
    x = lax.axis_index("tp")
    plane = me // 8
    place = lax.rem(me, 8)
    row = place // 2
    core = lax.rem(place, 2)
    right = lax.rem(x + 1, 4)
    left = lax.rem(x + 3, 4)
    across = lax.rem(x + 2, 4)
    partner = {"ep": 31 - me}
    guests = jnp.maximum(SHARE - 1 - me, 0)
    near = jnp.minimum(me, SHARE)
    bf16, f32 = jnp.bfloat16, jnp.float32

    loads = [
        pltpu.make_async_copy(src, dst, w_sem.at[i])
        for i, (src, dst) in enumerate(
            ((wg_any.at[0], wg), (wu_any.at[0], wu), (wd_any.at[0], wd), (ow_any, ow))
        )
    ]
    for load in loads:
        load.start()

    barrier = pltpu.get_barrier_semaphore()

    def greet(i, _):
        pl.semaphore_signal(
            barrier, inc=1, device_id={"ep": lax.rem(me + i, 32)}, device_id_type=MESH
        )
        return 0

    lax.fori_loop(1, 32, greet, 0)
    for side in (left, right, across):
        pl.semaphore_signal(barrier, inc=1, device_id={"tp": side}, device_id_type=MESH)

    def clear(i, _):
        kt[i, pl.ds(144, 112), :] = jnp.zeros((112, BLK), bf16)
        return 0

    lax.fori_loop(0, 32, clear, 0)
    own = plane * 8 + core * 4 + row
    kt[own, pl.ds(0, 128), :] = key_ref[...].astype(f32).T.astype(bf16)
    bias = bias_ref[...].astype(f32) * 8.0
    sub = iota((16, BLK), 0)
    extra = jnp.where(sub == 0, bias[0:1, :], jnp.where(sub == 1, bias[1:2, :], 0.0))
    extra = jnp.where((sub >= 2) & (sub <= 4), 1.0, extra)
    kt[own, pl.ds(128, 16), :] = extra.astype(bf16)
    vv[own, :, pl.ds(0, 128)] = value_ref[pl.ds(0, 128), :]
    vv[own, :, pl.ds(128, 128)] = value_ref[pl.ds(128, 128), :]

    expert_at = iota((32, 128), 0)
    earlier = jnp.where(iota((128, 128), 0) < iota((128, 128), 1), 1.0, 0.0).astype(bf16)
    base = (expert_at * CAP).astype(f32)
    slots = []
    for c in range(2):
        named = expert_at == routes_ref[c : c + 1, :]
        count = jnp.where(named, 1.0, 0.0)
        rank = base + jnp.dot(count.astype(bf16), earlier, preferred_element_type=f32)
        slots.append(jnp.sum(jnp.where(named, rank, 0.0), axis=0, keepdims=True).astype(jnp.int32))
        base = base + jnp.sum(count, axis=1, keepdims=True)
    slot_at = iota((32 * CAP, 128), 0)

    def norm(i, _):
        at = pl.ds(pl.multiple_of(i * 32, 32), 32)
        values = x_ref[at, :].astype(f32)
        scale = lax.rsqrt(jnp.mean(values * values, axis=1, keepdims=True) + EPSILON)
        xs[at, :] = (values * scale * gain_ref[...]).astype(bf16)
        return 0

    lax.fori_loop(0, 4, norm, 0)
    pick = jnp.where((slot_at == slots[0]) | (slot_at == slots[1]), 1.0, 0.0).astype(bf16)

    def dispatch(i, _):
        at = pl.ds(pl.multiple_of(i * 256, 256), 256)
        rows = jnp.dot(pick, xs[pl.ds(0, 128), at], preferred_element_type=f32)
        o4[:, :, at] = rows.astype(bf16).reshape(96, 4, 256)
        return 0

    lax.fori_loop(0, 8, dispatch, 0)
    rx[0, pl.ds(place * 3, 3)] = o4[pl.ds(me * 3, 3)]
    pl.semaphore_wait(barrier, 34)

    def along_y(d):
        return {"ep": plane * 8 + lax.rem(row + d, 4) * 2 + core}

    def along_z(d):
        return {"ep": lax.rem(plane + d, 4) * 8 + place}

    def kt_y(d):
        return kt.at[plane * 8 + core * 4 + lax.rem(row + d, 4), pl.ds(0, 144)]

    def vv_y(d):
        return vv.at[plane * 8 + core * 4 + lax.rem(row + d, 4)]

    def kt_z(d, c=core):
        return kt.at[pl.ds(lax.rem(plane + d, 4) * 8 + c * 4, 4), pl.ds(0, 144)]

    def vv_z(d, c=core):
        return vv.at[pl.ds(lax.rem(plane + d, 4) * 8 + c * 4, 4)]

    def keys_y():
        for s, d in enumerate((1, 3)):
            remote(kt_y(0), kt_y(0), ky_send.at[s, 0], ky_recv.at[s, 0], along_y(d))
            remote(vv_y(0), vv_y(0), ky_send.at[s, 1], ky_recv.at[s, 1], along_y(d))

    def keys_y_on():
        arrived(kt_y(3), ky_recv.at[0, 0])
        remote(kt_y(3), kt_y(3), ky_send.at[2, 0], ky_recv.at[2, 0], along_y(1))
        arrived(vv_y(1), ky_recv.at[1, 1])
        remote(vv_y(1), vv_y(1), ky_send.at[2, 1], ky_recv.at[2, 1], along_y(3))
        arrived(vv_y(3), ky_recv.at[0, 1])
        arrived(kt_y(1), ky_recv.at[1, 0])

    def keys_z():
        arrived(kt_y(2), ky_recv.at[2, 0])
        arrived(vv_y(2), ky_recv.at[2, 1])
        for s, d in enumerate((1, 3)):
            remote(kt_z(0), kt_z(0), kz_send.at[s, 0], kz_recv.at[s, 0], along_z(d))
            remote(vv_z(0), vv_z(0), kz_send.at[s, 1], kz_recv.at[s, 1], along_z(d))

    def keys_z_on():
        arrived(kt_z(3), kz_recv.at[0, 0])
        remote(kt_z(3), kt_z(3), kz_send.at[2, 0], kz_recv.at[2, 0], along_z(1))
        arrived(vv_z(1), kz_recv.at[1, 1])
        remote(vv_z(1), vv_z(1), kz_send.at[2, 1], kz_recv.at[2, 1], along_z(3))
        arrived(vv_z(3), kz_recv.at[0, 1])
        arrived(kt_z(1), kz_recv.at[1, 0])

    def keys_core():
        arrived(kt_z(2), kz_recv.at[2, 0])
        arrived(vv_z(2), kz_recv.at[2, 1])
        for d in range(4):
            device = {"ep": me + 1 - 2 * core}
            remote(kt_z(d), kt_z(d), kc_send.at[d, 0], kc_recv.at[d, 0], device)
            remote(vv_z(d), vv_z(d), kc_send.at[d, 1], kc_recv.at[d, 1], device)

    def keys_here():
        for d in range(4):
            arrived(kt_z(d, 1 - core), kc_recv.at[d, 0])
            arrived(vv_z(d, 1 - core), kc_recv.at[d, 1])

    for k, off in enumerate(OFFSETS):
        far = lax.rem(plane + off, 4) * 8

        def send_rows(i, _, k=k, far=far):
            j = lax.rem(place + i, 8)
            remote(
                o4.at[pl.ds((far + j) * 3, 3)],
                rx.at[k, pl.ds(place * 3, 3)],
                a2a_send,
                a2a_recv.at[k],
                {"ep": far + j},
            )
            return 0

        lax.fori_loop(1 if k == 0 else 0, 8, send_rows, 0)

    keys_y()

    @pl.when(me >= SHARE)
    def _():
        remote(query_ref, guest, pair_send.at[0], pair_recv.at[0], partner)

    def gather_start(k):
        if k == 0:
            arrived(rx.at[0, pl.ds(0, 21)], a2a_recv.at[0])
        else:
            arrived(rx.at[k, pl.ds(0, 24)], a2a_recv.at[k])
        own = rx.at[k, pl.ds(0, 24)]
        remote(own, rx.at[k, pl.ds(24, 24)], ag_send.at[k, 0], ag_recv.at[k, 0], {"tp": right})
        remote(own, rx.at[k, pl.ds(48, 24)], ag_send.at[k, 1], ag_recv.at[k, 1], {"tp": left})

    def gather_forward(k):
        arrived(rx.at[k, pl.ds(24, 24)], ag_recv.at[k, 0])
        remote(
            rx.at[k, pl.ds(24, 12)],
            rx.at[k, pl.ds(72, 12)],
            fw_send.at[k, 0],
            fw_recv.at[k, 0],
            {"tp": right},
        )
        arrived(rx.at[k, pl.ds(48, 24)], ag_recv.at[k, 1])
        remote(
            rx.at[k, pl.ds(60, 12)],
            rx.at[k, pl.ds(84, 12)],
            fw_send.at[k, 1],
            fw_recv.at[k, 1],
            {"tp": left},
        )

    def expert(k):
        if k == 0:
            for load in loads[:3]:
                load.wait()
        arrived(rx.at[k, pl.ds(72, 12)], fw_recv.at[k, 0])
        arrived(rx.at[k, pl.ds(84, 12)], fw_recv.at[k, 1])

        def unpack(i, _):
            xs[pl.ds(pl.multiple_of(i * 32, 32), 32), :] = rx[k, pl.ds(i * 8, 8)].reshape(32, 2048)
            return 0

        lax.fori_loop(0, 12, unpack, 0)

        def hidden(at, width):
            rows = xs[...]
            gate = jnp.dot(rows, wg[:, pl.ds(at, width)], preferred_element_type=jnp.float32)
            up = jnp.dot(rows, wu[:, pl.ds(at, width)], preferred_element_type=jnp.float32)
            hs[:, pl.ds(at, width)] = (gate / (1.0 + jnp.exp(-gate)) * up).astype(jnp.bfloat16)

        def hidden_tile(i, _):
            hidden(pl.multiple_of(i * 256, 256), 256)
            return 0

        lax.fori_loop(0, 3, hidden_tile, 0)
        hidden(768, 128)

        def down(i, _):
            at = pl.multiple_of(i * 256, 256)
            part = jnp.dot(hs[...], wd[:, pl.ds(at, 256)], preferred_element_type=jnp.float32)
            ys[k, :, :, pl.ds(at, 256)] = part.astype(jnp.bfloat16).reshape(96, 4, 256)
            return 0

        lax.fori_loop(0, 8, down, 0)
        remote(
            ys.at[k, pl.ds(72, 12)],
            first.at[k, 0],
            r1_send.at[k, 0],
            r1_recv.at[k, 0],
            {"tp": right},
        )
        remote(
            ys.at[k, pl.ds(84, 12)],
            first.at[k, 1],
            r1_send.at[k, 1],
            r1_recv.at[k, 1],
            {"tp": left},
        )
        remote(
            ys.at[k, pl.ds(60, 12)],
            fin.at[k, 0, pl.ds(12, 12)],
            rd_send.at[k, 0],
            fin_recv.at[k, 0],
            {"tp": right},
        )
        remote(
            ys.at[k, pl.ds(24, 12)],
            fin.at[k, 1, pl.ds(0, 12)],
            rd_send.at[k, 1],
            fin_recv.at[k, 1],
            {"tp": left},
        )

    def added(k):
        for side, at, device in ((0, 48, right), (1, 36, left)):
            arrived(first.at[k, side], r1_recv.at[k, side])

            def add(i, _, side=side, at=at):
                both = ys[k, pl.ds(at + 2 * i, 2)].astype(jnp.float32) + first[
                    k, side, pl.ds(2 * i, 2)
                ].astype(jnp.float32)
                mid[k, side, pl.ds(2 * i, 2)] = both.astype(jnp.bfloat16)
                return 0

            lax.fori_loop(0, 6, add, 0)
            remote(
                mid.at[k, side],
                fin.at[k, side, pl.ds(12 * side, 12)],
                rm_send.at[k, side],
                fin_recv.at[k, 2 + side],
                {"tp": device},
            )

    def back(k):
        arrived(fin.at[k, 0, pl.ds(12, 12)], fin_recv.at[k, 0])
        arrived(fin.at[k, 1, pl.ds(0, 12)], fin_recv.at[k, 1])
        arrived(fin.at[k, 0, pl.ds(0, 12)], fin_recv.at[k, 2])
        arrived(fin.at[k, 1, pl.ds(12, 12)], fin_recv.at[k, 3])

        def add(i, _):
            total = ys[k, pl.ds(2 * i, 2)].astype(jnp.float32)
            total = total + fin[k, 0, pl.ds(2 * i, 2)].astype(jnp.float32)
            total = total + fin[k, 1, pl.ds(2 * i, 2)].astype(jnp.float32)
            res[k, pl.ds(2 * i, 2)] = total.astype(jnp.bfloat16)
            return 0

        lax.fori_loop(0, 12, add, 0)
        far = lax.rem(plane + 4 - OFFSETS[k], 4) * 8

        def send_back(i, _):
            j = lax.rem(place + i, 8)
            remote(
                res.at[k, pl.ds(j * 3, 3)],
                r4.at[pl.ds(me * 3, 3)],
                ret_send,
                ret_recv.at[k],
                {"ep": far + j},
            )
            return 0

        lax.fori_loop(1 if k == 0 else 0, 8, send_back, 0)
        if k == 0:
            r4[pl.ds(me * 3, 3)] = res[0, pl.ds(place * 3, 3)]

    def queries(source):
        lane = iota((1, 128), 1)
        half = iota((BLK, 128), 1) < HD
        for g in range(2):
            for j in range(4):
                h = 4 * g + j
                pair = source[:, 128 * (h // 2) : 128 * (h // 2 + 1)].astype(f32)
                if h % 2 != g:
                    pair = pltpu.roll(pair, HD, 1)
                qa[g, pl.ds(BLK * j, BLK), pl.ds(0, 128)] = jnp.where(
                    half if g == 0 else ~half, pair, 0.0
                ).astype(bf16)
                rest = jnp.full((1, 128), offset_ref[h] * 8.0, f32)
                columns = jnp.where(lane == g, 1.0, 0.0)
                for t in range(3):
                    term = rest.astype(bf16).astype(f32)
                    columns = jnp.where(lane == 2 + t, term, columns)
                    rest = rest - term
                qa[g, pl.ds(BLK * j, BLK), pl.ds(128, 128)] = jnp.broadcast_to(
                    columns, (BLK, 128)
                ).astype(bf16)
        acc[...] = jnp.zeros_like(acc)
        surv[...] = jnp.zeros_like(surv)

    def block(index, diagonal):
        at = (index // 8) * 8 + lax.rem(index, 2) * 4 + lax.rem(index, 8) // 2
        keys = kt[at]
        for g in range(2):
            vals = jnp.concatenate(
                [
                    vv[at, :, HD * g : HD * (g + 1)],
                    vv[at, :, 128 + HD * g : 128 + HD * (g + 1)],
                ],
                axis=0,
            )
            for m in range(4 * BLK // TILE):
                part = slice(m * TILE, (m + 1) * TILE)
                z = jnp.dot(qa[g, part, :], keys, preferred_element_type=f32) * TO_LOG2
                if diagonal:
                    z = jnp.where(
                        iota((TILE, BLK), 1) < lax.rem(iota((TILE, BLK), 0), BLK), z, -1e30
                    )
                leave = jnp.maximum(z, jnp.log2(1.0 + jnp.exp2(jnp.minimum(z, 100.0))))
                after = jnp.dot(leave.astype(bf16), tri[...], preferred_element_type=f32) - leave
                s = surv[g, part, :]
                w = jnp.exp2(z + after + jnp.concatenate([s, s], axis=1)).astype(bf16)
                acc[g, part, :] += jnp.dot(w, vals, preferred_element_type=f32)
                surv[g, part, :] = s + jnp.broadcast_to(after[:, 0:1], s.shape)

    def attend_start():
        tri[...] = jnp.where(iota((BLK, BLK), 0) > iota((BLK, BLK), 1), -1.0, 0.0).astype(bf16)

        @pl.when(me < SHARE)
        def _():
            arrived(guest, pair_recv.at[0])
            queries(guest)

    def own_start():
        @pl.when(me < SHARE)
        def _():
            far_out[...] = jnp.concatenate([acc[0], acc[1]], axis=1).astype(bf16)
            remote(far_out, far_in, pair_send.at[1], pair_recv.at[1], partner)

        queries(query_ref)
        block(me, True)

    def attend(begin, end):
        def step(i, _):
            @pl.when(i == guests)
            def _():
                own_start()

            @pl.when(i != guests)
            def _():
                block(jnp.where(i < guests, SHARE - 2 - me - i, me + guests - i), False)

            return 0

        lax.fori_loop(
            jnp.minimum(begin, guests + 1 + near), jnp.minimum(end, guests + 1 + near), step, 0
        )

    def project():
        @pl.when(me >= SHARE)
        def _():
            arrived(far_in, pair_recv.at[1])
            for g in range(2):
                far = far_in[:, HD * g : HD * (g + 1)].astype(f32)
                acc[g] += jnp.exp2(surv[g, :, 0:HD]) * far

        for h in range(0, 8, 2):
            pair = [
                acc[(h + i) // 4, pl.ds(BLK * ((h + i) % 4), BLK), :].astype(bf16)
                for i in range(2)
            ]
            ho[:, pl.ds(HD * h, 2 * HD)] = jnp.concatenate(pair, axis=1)
        loads[3].wait()

        def out(i, _):
            at = pl.ds(pl.multiple_of(i * 256, 256), 256)
            part = jnp.dot(ho[...], ow[:, at], preferred_element_type=f32).astype(bf16)
            po[:, :, at] = part.reshape(4, 64, 256)
            return 0

        lax.fori_loop(0, 8, out, 0)
        for s, side in enumerate((across, right, left)):
            remote(po.at[side], pm.at[s], po_send.at[s], po_recv.at[s], {"tp": side})

    def mixed():
        for s in range(3):
            arrived(pm.at[s], po_recv.at[s])
        total = po[x].astype(f32)
        for s in range(3):
            total = total + pm[s].astype(f32)
        mixed_a_ref[...] = total.astype(bf16)

    gather_start(0)
    gather_start(1)
    keys_y_on()
    gather_start(2)
    gather_forward(0)
    keys_z()
    gather_start(3)
    gather_forward(1)
    keys_z_on()
    expert(0)
    keys_core()
    gather_forward(2)
    expert(1)
    added(0)
    gather_forward(3)
    expert(2)
    added(1)
    back(0)
    expert(3)
    added(2)
    keys_here()
    attend_start()
    attend(0, 4)
    added(3)
    attend(4, 8)
    back(1)
    attend(8, 13)
    back(2)
    attend(13, 15)
    back(3)
    attend(15, 17)
    project()

    arrived(o4.at[pl.ds(0, 93)], a2a_send)
    for k in range(4):
        for side in range(2):
            arrived(rx.at[k, pl.ds(0, 24)], ag_send.at[k, side])
            arrived(rx.at[k, pl.ds(24, 12)], fw_send.at[k, side])
            arrived(first.at[k, side], r1_send.at[k, side])
            arrived(first.at[k, side], rd_send.at[k, side])
            arrived(first.at[k, side], rm_send.at[k, side])
    for s in range(3):
        arrived(kt_y(0), ky_send.at[s, 0])
        arrived(vv_y(0), ky_send.at[s, 1])
        arrived(kt_z(0), kz_send.at[s, 0])
        arrived(vv_z(0), kz_send.at[s, 1])
    for d in range(4):
        arrived(kt_z(0), kc_send.at[d, 0])
        arrived(vv_z(0), kc_send.at[d, 1])
    arrived(o4.at[pl.ds(0, 93)], ret_send)

    for k in range(4):
        arrived(r4.at[pl.ds(0, 21 if k == 0 else 24)], ret_recv.at[k])
        far = lax.rem(plane + OFFSETS[k], 4) * 24

        def unpack_back(i, _, far=far):
            at = far + i * 8
            xs[pl.ds(pl.multiple_of(at * 4, 32), 32), :] = r4[pl.ds(at, 8)].reshape(32, 2048)
            return 0

        lax.fori_loop(0, 3, unpack_back, 0)

    weight = jnp.where(slot_at == slots[0], rw_ref[0:1, :], 0.0)
    weight = weight + jnp.where(slot_at == slots[1], rw_ref[1:2, :], 0.0)
    high = weight.astype(bf16)
    low = (weight - high.astype(f32)).astype(bf16)

    def combine(i, _):
        at = pl.ds(pl.multiple_of(i * 256, 256), 256)
        rows = xs[:, at]
        dims = (((0,), (0,)), ((), ()))
        total = lax.dot_general(high, rows, dims, preferred_element_type=f32)
        total = total + lax.dot_general(low, rows, dims, preferred_element_type=f32)
        mixed_b_ref[:, at] = total.astype(bf16)
        return 0

    lax.fori_loop(0, 8, combine, 0)
    mixed()
    for s in range(3):
        arrived(pm.at[s], po_send.at[s])

    @pl.when(me >= SHARE)
    def _():
        arrived(guest, pair_send.at[0])

    @pl.when(me < SHARE)
    def _():
        arrived(far_in, pair_send.at[1])


def body(
    query_rows,
    key_rows,
    value_rows,
    key_bias,
    head_offset,
    out_weight,
    expert_input,
    expert_gain,
    routes,
    route_weight,
    gate_weight,
    up_weight,
    down_weight,
):
    width, ff = gate_weight.shape[1:]
    tokens = expert_input.shape[0]
    rows = 32 * CAP
    bf16, f32 = jnp.bfloat16, jnp.float32
    dma = pltpu.SemaphoreType.DMA
    vmem = pltpu.VMEM
    here, there = pl.BlockSpec(memory_space=vmem), pl.BlockSpec(memory_space=pl.ANY)
    return pl.pallas_call(
        step_kernel,
        out_shape=(
            jax.ShapeDtypeStruct((BLK // 4, width), bf16),
            jax.ShapeDtypeStruct((tokens, width), bf16),
        ),
        in_specs=[here] * 4
        + [pl.BlockSpec(memory_space=pltpu.SMEM)]
        + [here] * 4
        + [there] * 4,
        out_specs=(here, here),
        scratch_shapes=[
            vmem((8 * HD, width), bf16),
            vmem((width, ff), bf16),
            vmem((width, ff), bf16),
            vmem((ff, width), bf16),
            vmem((96, 4, width), bf16),
            vmem((4, 96, 4, width), bf16),
            vmem((4, 96, 4, width), bf16),
            vmem((4, 2, 12, 4, width), bf16),
            vmem((4, 2, 12, 4, width), bf16),
            vmem((4, 2, 24, 4, width), bf16),
            vmem((4, 24, 4, width), bf16),
            vmem((96, 4, width), bf16),
            vmem((rows, width), bf16),
            vmem((rows, ff), bf16),
            vmem((32, BLK, BLK), bf16),
            vmem((32, BLK // 2, BLK), bf16),
            vmem((2, 4 * BLK, 256), bf16),
            vmem((2, 4 * BLK, HD), f32),
            vmem((2, 4 * BLK, 128), f32),
            vmem((BLK, BLK), bf16),
            vmem((BLK, 8 * HD), bf16),
            vmem((4, BLK // 4, width), bf16),
            vmem((3, BLK // 4, width), bf16),
            dma((4,)),
            dma,
            dma((4,)),
            dma((4, 2)),
            dma((4, 2)),
            dma((4, 2)),
            dma((4, 2)),
            dma((4, 2)),
            dma((4, 2)),
            dma((4, 2)),
            dma((4, 2)),
            dma((4, 4)),
            dma,
            dma((4,)),
            dma((3, 2)),
            dma((3, 2)),
            dma((3, 2)),
            dma((3, 2)),
            dma((4, 2)),
            dma((4, 2)),
            dma((3,)),
            dma((3,)),
            vmem((BLK, 8 * HD), bf16),
            vmem((4 * BLK, 2 * HD), bf16),
            vmem((4 * BLK, 2 * HD), bf16),
            dma((2,)),
            dma((2,)),
        ],
        compiler_params=pltpu.CompilerParams(
            vmem_limit_bytes=63 * 1024 * 1024, collective_id=0, has_side_effects=True
        ),
        name="step",
    )(
        query_rows,
        key_rows,
        value_rows,
        key_bias.T,
        head_offset,
        expert_input,
        expert_gain[None, :],
        routes.T,
        route_weight.T,
        out_weight,
        gate_weight,
        up_weight,
        down_weight,
    )


def solution(mesh):
    return jax.shard_map(
        body,
        mesh=mesh,
        in_specs=(
            P("ep", "tp"),
            P("ep", "tp"),
            P("ep", "tp"),
            P("ep", "tp"),
            P("tp"),
            P("tp", None),
            P(("ep", "tp"), None),
            P(),
            P(("ep", "tp"), None),
            P(("ep", "tp"), None),
            P("ep", None, "tp"),
            P("ep", None, "tp"),
            P("ep", "tp", None),
        ),
        out_specs=(P(("ep", "tp"), None), P(("ep", "tp"), None)),
        check_vma=False,
    )
```

```python
import math

import jax
import jax.numpy as jnp
from jax import lax
from jax.experimental import pallas as pl
from jax.experimental.pallas import tpu as pltpu
from jax.sharding import PartitionSpec as P

HD = 64
BLK = 256
CAP = 12
EPSILON = 1e-06
TO_LOG2 = math.log2(math.e) / math.sqrt(HD)
OFFSETS = (0, 1, 3, 2)
SHARE = 16
TILE = 512
MESH = pl.DeviceIdType.MESH


def arrived(ref, sem):
    pltpu.make_async_copy(ref, ref, sem).wait()


def remote(src, dst, send, recv, device):
    pltpu.make_async_remote_copy(
        src_ref=src,
        dst_ref=dst,
        send_sem=send,
        recv_sem=recv,
        device_id=device,
        device_id_type=MESH,
    ).start()


def iota(shape, dim):
    return lax.broadcasted_iota(jnp.int32, shape, dim)


def step_kernel(
    query_ref,
    key_ref,
    value_ref,
    bias_ref,
    offset_ref,
    x_ref,
    gain_ref,
    routes_ref,
    rw_ref,
    ow_any,
    wg_any,
    wu_any,
    wd_any,
    mixed_a_ref,
    mixed_b_ref,
    ow,
    wg,
    wu,
    wd,
    o4,
    rx,
    ys,
    first,
    mid,
    fin,
    res,
    r4,
    xs,
    hs,
    kt,
    vv,
    qa,
    acc,
    surv,
    tri,
    ho,
    po,
    pm,
    w_sem,
    a2a_send,
    a2a_recv,
    ag_send,
    ag_recv,
    fw_send,
    fw_recv,
    r1_send,
    r1_recv,
    rd_send,
    rm_send,
    fin_recv,
    ret_send,
    ret_recv,
    ky_send,
    ky_recv,
    kz_send,
    kz_recv,
    kc_send,
    kc_recv,
    po_send,
    po_recv,
    guest,
    far_out,
    far_in,
    pair_send,
    pair_recv,
    near_out,
    nb_send,
    nb_recv,
):
    me = lax.axis_index("ep")
    x = lax.axis_index("tp")
    plane = me // 8
    place = lax.rem(me, 8)
    row = place // 2
    core = lax.rem(place, 2)
    right = lax.rem(x + 1, 4)
    left = lax.rem(x + 3, 4)
    across = lax.rem(x + 2, 4)
    partner = {"ep": 31 - me}
    guests = jnp.maximum(SHARE - 1 - me, 0)
    near = jnp.minimum(me, SHARE)
    bf16, f32 = jnp.bfloat16, jnp.float32

    loads = [
        pltpu.make_async_copy(src, dst, w_sem.at[i])
        for i, (src, dst) in enumerate(
            ((wg_any.at[0], wg), (wu_any.at[0], wu), (wd_any.at[0], wd), (ow_any, ow))
        )
    ]
    for load in loads:
        load.start()

    barrier = pltpu.get_barrier_semaphore()

    def greet(i, _):
        pl.semaphore_signal(
            barrier, inc=1, device_id={"ep": lax.rem(me + i, 32)}, device_id_type=MESH
        )
        return 0

    lax.fori_loop(1, 32, greet, 0)
    for side in (left, right, across):
        pl.semaphore_signal(barrier, inc=1, device_id={"tp": side}, device_id_type=MESH)

    def clear(i, _):
        kt[i, pl.ds(144, 112), :] = jnp.zeros((112, BLK), bf16)
        return 0

    lax.fori_loop(0, 32, clear, 0)
    own = plane * 8 + core * 4 + row
    kt[own, pl.ds(0, 128), :] = key_ref[...].astype(f32).T.astype(bf16)
    bias = bias_ref[...].astype(f32) * 8.0
    sub = iota((16, BLK), 0)
    extra = jnp.where(sub == 0, bias[0:1, :], jnp.where(sub == 1, bias[1:2, :], 0.0))
    extra = jnp.where((sub >= 2) & (sub <= 4), 1.0, extra)
    kt[own, pl.ds(128, 16), :] = extra.astype(bf16)
    vv[own, :, pl.ds(0, 128)] = value_ref[pl.ds(0, 128), :]
    vv[own, :, pl.ds(128, 128)] = value_ref[pl.ds(128, 128), :]

    expert_at = iota((32, 128), 0)
    earlier = jnp.where(iota((128, 128), 0) < iota((128, 128), 1), 1.0, 0.0).astype(bf16)
    base = (expert_at * CAP).astype(f32)
    slots = []
    for c in range(2):
        named = expert_at == routes_ref[c : c + 1, :]
        count = jnp.where(named, 1.0, 0.0)
        rank = base + jnp.dot(count.astype(bf16), earlier, preferred_element_type=f32)
        slots.append(jnp.sum(jnp.where(named, rank, 0.0), axis=0, keepdims=True).astype(jnp.int32))
        base = base + jnp.sum(count, axis=1, keepdims=True)
    slot_at = iota((32 * CAP, 128), 0)

    def norm(i, _):
        at = pl.ds(pl.multiple_of(i * 32, 32), 32)
        values = x_ref[at, :].astype(f32)
        scale = lax.rsqrt(jnp.mean(values * values, axis=1, keepdims=True) + EPSILON)
        xs[at, :] = (values * scale * gain_ref[...]).astype(bf16)
        return 0

    lax.fori_loop(0, 4, norm, 0)
    pick = jnp.where((slot_at == slots[0]) | (slot_at == slots[1]), 1.0, 0.0).astype(bf16)

    def dispatch(i, _):
        at = pl.ds(pl.multiple_of(i * 256, 256), 256)
        rows = jnp.dot(pick, xs[pl.ds(0, 128), at], preferred_element_type=f32)
        o4[:, :, at] = rows.astype(bf16).reshape(96, 4, 256)
        return 0

    lax.fori_loop(0, 8, dispatch, 0)
    rx[0, pl.ds(place * 3, 3)] = o4[pl.ds(me * 3, 3)]
    pl.semaphore_wait(barrier, 34)

    def along_y(d):
        return {"ep": plane * 8 + lax.rem(row + d, 4) * 2 + core}

    def along_z(d):
        return {"ep": lax.rem(plane + d, 4) * 8 + place}

    def kt_y(d):
        return kt.at[plane * 8 + core * 4 + lax.rem(row + d, 4), pl.ds(0, 144)]

    def vv_y(d):
        return vv.at[plane * 8 + core * 4 + lax.rem(row + d, 4)]

    def kt_z(d, c=core):
        return kt.at[pl.ds(lax.rem(plane + d, 4) * 8 + c * 4, 4), pl.ds(0, 144)]

    def vv_z(d, c=core):
        return vv.at[pl.ds(lax.rem(plane + d, 4) * 8 + c * 4, 4)]

    def keys_y():
        for s, d in enumerate((1, 3)):
            remote(kt_y(0), kt_y(0), ky_send.at[s, 0], ky_recv.at[s, 0], along_y(d))
            remote(vv_y(0), vv_y(0), ky_send.at[s, 1], ky_recv.at[s, 1], along_y(d))

    def keys_y_on():
        arrived(kt_y(3), ky_recv.at[0, 0])
        remote(kt_y(3), kt_y(3), ky_send.at[2, 0], ky_recv.at[2, 0], along_y(1))
        arrived(vv_y(1), ky_recv.at[1, 1])
        remote(vv_y(1), vv_y(1), ky_send.at[2, 1], ky_recv.at[2, 1], along_y(3))
        arrived(vv_y(3), ky_recv.at[0, 1])
        arrived(kt_y(1), ky_recv.at[1, 0])

    def keys_z():
        arrived(kt_y(2), ky_recv.at[2, 0])
        arrived(vv_y(2), ky_recv.at[2, 1])
        for s, d in enumerate((1, 3)):
            remote(kt_z(0), kt_z(0), kz_send.at[s, 0], kz_recv.at[s, 0], along_z(d))
            remote(vv_z(0), vv_z(0), kz_send.at[s, 1], kz_recv.at[s, 1], along_z(d))

    def keys_z_on():
        arrived(kt_z(3), kz_recv.at[0, 0])
        remote(kt_z(3), kt_z(3), kz_send.at[2, 0], kz_recv.at[2, 0], along_z(1))
        arrived(vv_z(1), kz_recv.at[1, 1])
        remote(vv_z(1), vv_z(1), kz_send.at[2, 1], kz_recv.at[2, 1], along_z(3))
        arrived(vv_z(3), kz_recv.at[0, 1])
        arrived(kt_z(1), kz_recv.at[1, 0])

    def keys_core():
        arrived(kt_z(2), kz_recv.at[2, 0])
        arrived(vv_z(2), kz_recv.at[2, 1])
        for d in range(4):
            device = {"ep": me + 1 - 2 * core}
            remote(kt_z(d), kt_z(d), kc_send.at[d, 0], kc_recv.at[d, 0], device)
            remote(vv_z(d), vv_z(d), kc_send.at[d, 1], kc_recv.at[d, 1], device)

    def keys_here():
        for d in range(4):
            arrived(kt_z(d, 1 - core), kc_recv.at[d, 0])
            arrived(vv_z(d, 1 - core), kc_recv.at[d, 1])

    for k, off in enumerate(OFFSETS):
        far = lax.rem(plane + off, 4) * 8

        def send_rows(i, _, k=k, far=far):
            j = lax.rem(place + i, 8)
            remote(
                o4.at[pl.ds((far + j) * 3, 3)],
                rx.at[k, pl.ds(place * 3, 3)],
                a2a_send,
                a2a_recv.at[k],
                {"ep": far + j},
            )
            return 0

        lax.fori_loop(1 if k == 0 else 0, 8, send_rows, 0)

    keys_y()

    @pl.when(me >= SHARE)
    def _():
        remote(query_ref, guest, pair_send.at[0], pair_recv.at[0], partner)

    def gather_start(k):
        arrived(rx.at[k, pl.ds(0, 21 if k == 0 else 24)], a2a_recv.at[k])
        own = rx.at[k, pl.ds(0, 24)]
        remote(own, rx.at[k, pl.ds(24, 24)], ag_send.at[k, 0], ag_recv.at[k, 0], {"tp": right})
        remote(own, rx.at[k, pl.ds(48, 24)], ag_send.at[k, 1], ag_recv.at[k, 1], {"tp": left})

    def gather_forward(k):
        arrived(rx.at[k, pl.ds(24, 24)], ag_recv.at[k, 0])
        remote(
            rx.at[k, pl.ds(24, 12)],
            rx.at[k, pl.ds(72, 12)],
            fw_send.at[k, 0],
            fw_recv.at[k, 0],
            {"tp": right},
        )
        arrived(rx.at[k, pl.ds(48, 24)], ag_recv.at[k, 1])
        remote(
            rx.at[k, pl.ds(60, 12)],
            rx.at[k, pl.ds(84, 12)],
            fw_send.at[k, 1],
            fw_recv.at[k, 1],
            {"tp": left},
        )

    def expert(k):
        if k == 0:
            for load in loads[:3]:
                load.wait()
        arrived(rx.at[k, pl.ds(72, 12)], fw_recv.at[k, 0])
        arrived(rx.at[k, pl.ds(84, 12)], fw_recv.at[k, 1])

        def unpack(i, _):
            xs[pl.ds(pl.multiple_of(i * 32, 32), 32), :] = rx[k, pl.ds(i * 8, 8)].reshape(32, 2048)
            return 0

        lax.fori_loop(0, 12, unpack, 0)

        def hidden(at, width):
            rows = xs[...]
            gate = jnp.dot(rows, wg[:, pl.ds(at, width)], preferred_element_type=jnp.float32)
            up = jnp.dot(rows, wu[:, pl.ds(at, width)], preferred_element_type=jnp.float32)
            hs[:, pl.ds(at, width)] = (gate / (1.0 + jnp.exp(-gate)) * up).astype(jnp.bfloat16)

        def hidden_tile(i, _):
            hidden(pl.multiple_of(i * 256, 256), 256)
            return 0

        lax.fori_loop(0, 3, hidden_tile, 0)
        hidden(768, 128)

        def down(i, _):
            at = pl.multiple_of(i * 256, 256)
            part = jnp.dot(hs[...], wd[:, pl.ds(at, 256)], preferred_element_type=jnp.float32)
            ys[k, :, :, pl.ds(at, 256)] = part.astype(jnp.bfloat16).reshape(96, 4, 256)
            return 0

        lax.fori_loop(0, 8, down, 0)
        if k == 0:

            def send_near(i, _):
                j = lax.rem(place + i, 8)
                for c in range(4):
                    remote(
                        ys.at[0, pl.ds(24 * c + j * 3, 3)],
                        near_out.at[c, pl.ds(place * 3, 3)],
                        nb_send,
                        nb_recv,
                        {"ep": plane * 8 + j},
                    )
                return 0

            lax.fori_loop(1, 8, send_near, 0)
            for c in range(4):
                near_out[c, pl.ds(place * 3, 3)] = ys[0, pl.ds(24 * c + place * 3, 3)]
        else:
            reduce_start(k)

    def part(k, slot, at, count):
        if k == 0:
            return near_out.at[slot, pl.ds(at, count)]
        return ys.at[k, pl.ds(24 * slot + at, count)]

    def reduce_start(k):
        if k == 0:
            arrived(rx.at[0, pl.ds(0, 84)], nb_recv)
        remote(part(k, 3, 0, 12), first.at[k, 0], r1_send.at[k, 0], r1_recv.at[k, 0], {"tp": right})
        remote(part(k, 3, 12, 12), first.at[k, 1], r1_send.at[k, 1], r1_recv.at[k, 1], {"tp": left})
        remote(
            part(k, 2, 12, 12),
            fin.at[k, 0, pl.ds(12, 12)],
            rd_send.at[k, 0],
            fin_recv.at[k, 0],
            {"tp": right},
        )
        remote(
            part(k, 1, 0, 12),
            fin.at[k, 1, pl.ds(0, 12)],
            rd_send.at[k, 1],
            fin_recv.at[k, 1],
            {"tp": left},
        )

    def added(k):
        for side, slot, at, device in ((0, 2, 0, right), (1, 1, 12, left)):
            arrived(first.at[k, side], r1_recv.at[k, side])

            def add(i, _, side=side, slot=slot, at=at):
                both = part(k, slot, at + 2 * i, 2)[...].astype(jnp.float32) + first[
                    k, side, pl.ds(2 * i, 2)
                ].astype(jnp.float32)
                mid[k, side, pl.ds(2 * i, 2)] = both.astype(jnp.bfloat16)
                return 0

            lax.fori_loop(0, 6, add, 0)
            remote(
                mid.at[k, side],
                fin.at[k, side, pl.ds(12 * side, 12)],
                rm_send.at[k, side],
                fin_recv.at[k, 2 + side],
                {"tp": device},
            )

    def back(k):
        arrived(fin.at[k, 0, pl.ds(12, 12)], fin_recv.at[k, 0])
        arrived(fin.at[k, 1, pl.ds(0, 12)], fin_recv.at[k, 1])
        arrived(fin.at[k, 0, pl.ds(0, 12)], fin_recv.at[k, 2])
        arrived(fin.at[k, 1, pl.ds(12, 12)], fin_recv.at[k, 3])

        def add(i, _):
            total = part(k, 0, 2 * i, 2)[...].astype(jnp.float32)
            total = total + fin[k, 0, pl.ds(2 * i, 2)].astype(jnp.float32)
            total = total + fin[k, 1, pl.ds(2 * i, 2)].astype(jnp.float32)
            if k == 0:
                r4[pl.ds(plane * 24 + 2 * i, 2)] = total.astype(jnp.bfloat16)
            else:
                res[k, pl.ds(2 * i, 2)] = total.astype(jnp.bfloat16)
            return 0

        lax.fori_loop(0, 12, add, 0)
        if k == 0:
            return
        far = lax.rem(plane + 4 - OFFSETS[k], 4) * 8

        def send_back(i, _):
            j = lax.rem(place + i, 8)
            remote(
                res.at[k, pl.ds(j * 3, 3)],
                r4.at[pl.ds(me * 3, 3)],
                ret_send,
                ret_recv.at[k],
                {"ep": far + j},
            )
            return 0

        lax.fori_loop(0, 8, send_back, 0)

    def queries(source):
        lane = iota((1, 128), 1)
        half = iota((BLK, 128), 1) < HD
        for g in range(2):
            for j in range(4):
                h = 4 * g + j
                pair = source[:, 128 * (h // 2) : 128 * (h // 2 + 1)].astype(f32)
                if h % 2 != g:
                    pair = pltpu.roll(pair, HD, 1)
                qa[g, pl.ds(BLK * j, BLK), pl.ds(0, 128)] = jnp.where(
                    half if g == 0 else ~half, pair, 0.0
                ).astype(bf16)
                rest = jnp.full((1, 128), offset_ref[h] * 8.0, f32)
                columns = jnp.where(lane == g, 1.0, 0.0)
                for t in range(3):
                    term = rest.astype(bf16).astype(f32)
                    columns = jnp.where(lane == 2 + t, term, columns)
                    rest = rest - term
                qa[g, pl.ds(BLK * j, BLK), pl.ds(128, 128)] = jnp.broadcast_to(
                    columns, (BLK, 128)
                ).astype(bf16)
        acc[...] = jnp.zeros_like(acc)
        surv[...] = jnp.zeros_like(surv)

    def block(index, diagonal):
        at = (index // 8) * 8 + lax.rem(index, 2) * 4 + lax.rem(index, 8) // 2
        keys = kt[at]
        for g in range(2):
            vals = jnp.concatenate(
                [
                    vv[at, :, HD * g : HD * (g + 1)],
                    vv[at, :, 128 + HD * g : 128 + HD * (g + 1)],
                ],
                axis=0,
            )
            for m in range(4 * BLK // TILE):
                part = slice(m * TILE, (m + 1) * TILE)
                z = jnp.dot(qa[g, part, :], keys, preferred_element_type=f32) * TO_LOG2
                if diagonal:
                    z = jnp.where(
                        iota((TILE, BLK), 1) < lax.rem(iota((TILE, BLK), 0), BLK), z, -1e30
                    )
                leave = jnp.maximum(z, jnp.log2(1.0 + jnp.exp2(jnp.minimum(z, 100.0))))
                after = jnp.dot(leave.astype(bf16), tri[...], preferred_element_type=f32) - leave
                s = surv[g, part, :]
                w = jnp.exp2(z + after + jnp.concatenate([s, s], axis=1)).astype(bf16)
                acc[g, part, :] += jnp.dot(w, vals, preferred_element_type=f32)
                surv[g, part, :] = s + jnp.broadcast_to(after[:, 0:1], s.shape)

    def attend_start():
        tri[...] = jnp.where(iota((BLK, BLK), 0) > iota((BLK, BLK), 1), -1.0, 0.0).astype(bf16)

        @pl.when(me < SHARE)
        def _():
            arrived(guest, pair_recv.at[0])
            queries(guest)

    def own_start():
        @pl.when(me < SHARE)
        def _():
            far_out[...] = jnp.concatenate([acc[0], acc[1]], axis=1).astype(bf16)
            remote(far_out, far_in, pair_send.at[1], pair_recv.at[1], partner)

        queries(query_ref)
        block(me, True)

    def attend(begin, end):
        def step(i, _):
            @pl.when(i == guests)
            def _():
                own_start()

            @pl.when(i != guests)
            def _():
                block(jnp.where(i < guests, SHARE - 2 - me - i, me + guests - i), False)

            return 0

        lax.fori_loop(
            jnp.minimum(begin, guests + 1 + near), jnp.minimum(end, guests + 1 + near), step, 0
        )

    def project():
        @pl.when(me >= SHARE)
        def _():
            arrived(far_in, pair_recv.at[1])
            for g in range(2):
                far = far_in[:, HD * g : HD * (g + 1)].astype(f32)
                acc[g] += jnp.exp2(surv[g, :, 0:HD]) * far

        for h in range(0, 8, 2):
            pair = [
                acc[(h + i) // 4, pl.ds(BLK * ((h + i) % 4), BLK), :].astype(bf16)
                for i in range(2)
            ]
            ho[:, pl.ds(HD * h, 2 * HD)] = jnp.concatenate(pair, axis=1)
        loads[3].wait()

        def out(i, _):
            at = pl.ds(pl.multiple_of(i * 256, 256), 256)
            part = jnp.dot(ho[...], ow[:, at], preferred_element_type=f32).astype(bf16)
            po[:, :, at] = part.reshape(4, 64, 256)
            return 0

        lax.fori_loop(0, 8, out, 0)
        for s, side in enumerate((across, right, left)):
            remote(po.at[side], pm.at[s], po_send.at[s], po_recv.at[s], {"tp": side})

    def mixed():
        for s in range(3):
            arrived(pm.at[s], po_recv.at[s])
        total = po[x].astype(f32)
        for s in range(3):
            total = total + pm[s].astype(f32)
        mixed_a_ref[...] = total.astype(bf16)

    gather_start(0)
    gather_start(1)
    keys_y_on()
    gather_start(2)
    gather_forward(0)
    keys_z()
    gather_start(3)
    gather_forward(1)
    keys_z_on()
    expert(0)
    keys_core()
    gather_forward(2)
    expert(1)
    gather_forward(3)
    keys_here()
    attend_start()
    attend(0,2)
    expert(2)
    added(1)
    expert(3)
    added(2)
    attend(2,5)
    added(3)
    reduce_start(0)
    attend(5,8)
    back(1)
    attend(8,10)
    back(2)
    attend(10,13)
    added(0)
    back(3)
    attend(13,15)
    back(0)
    attend(15,17)
    project()

    arrived(o4.at[pl.ds(0, 93)], a2a_send)
    for k in range(4):
        for side in range(2):
            arrived(rx.at[k, pl.ds(0, 24)], ag_send.at[k, side])
            arrived(rx.at[k, pl.ds(24, 12)], fw_send.at[k, side])
            arrived(first.at[k, side], r1_send.at[k, side])
            arrived(first.at[k, side], rd_send.at[k, side])
            arrived(first.at[k, side], rm_send.at[k, side])
    for s in range(3):
        arrived(kt_y(0), ky_send.at[s, 0])
        arrived(vv_y(0), ky_send.at[s, 1])
        arrived(kt_z(0), kz_send.at[s, 0])
        arrived(vv_z(0), kz_send.at[s, 1])
    for d in range(4):
        arrived(kt_z(0), kc_send.at[d, 0])
        arrived(vv_z(0), kc_send.at[d, 1])
    arrived(o4.at[pl.ds(0, 72)], ret_send)
    arrived(rx.at[0, pl.ds(0, 84)], nb_send)

    for k in (1, 2, 3, 0):
        if k > 0:
            arrived(r4.at[pl.ds(0, 24)], ret_recv.at[k])
        far = lax.rem(plane + OFFSETS[k], 4) * 24

        def unpack_back(i, _, far=far):
            at = far + i * 8
            xs[pl.ds(pl.multiple_of(at * 4, 32), 32), :] = r4[pl.ds(at, 8)].reshape(32, 2048)
            return 0

        lax.fori_loop(0, 3, unpack_back, 0)

    weight = jnp.where(slot_at == slots[0], rw_ref[0:1, :], 0.0)
    weight = weight + jnp.where(slot_at == slots[1], rw_ref[1:2, :], 0.0)
    high = weight.astype(bf16)
    low = (weight - high.astype(f32)).astype(bf16)

    def combine(i, _):
        at = pl.ds(pl.multiple_of(i * 256, 256), 256)
        rows = xs[:, at]
        dims = (((0,), (0,)), ((), ()))
        total = lax.dot_general(high, rows, dims, preferred_element_type=f32)
        total = total + lax.dot_general(low, rows, dims, preferred_element_type=f32)
        mixed_b_ref[:, at] = total.astype(bf16)
        return 0

    lax.fori_loop(0, 8, combine, 0)
    mixed()
    for s in range(3):
        arrived(pm.at[s], po_send.at[s])

    @pl.when(me >= SHARE)
    def _():
        arrived(guest, pair_send.at[0])

    @pl.when(me < SHARE)
    def _():
        arrived(far_in, pair_send.at[1])


def body(
    query_rows,
    key_rows,
    value_rows,
    key_bias,
    head_offset,
    out_weight,
    expert_input,
    expert_gain,
    routes,
    route_weight,
    gate_weight,
    up_weight,
    down_weight,
):
    width, ff = gate_weight.shape[1:]
    tokens = expert_input.shape[0]
    rows = 32 * CAP
    bf16, f32 = jnp.bfloat16, jnp.float32
    dma = pltpu.SemaphoreType.DMA
    vmem = pltpu.VMEM
    here, there = pl.BlockSpec(memory_space=vmem), pl.BlockSpec(memory_space=pl.ANY)
    return pl.pallas_call(
        step_kernel,
        out_shape=(
            jax.ShapeDtypeStruct((BLK // 4, width), bf16),
            jax.ShapeDtypeStruct((tokens, width), bf16),
        ),
        in_specs=[here] * 4
        + [pl.BlockSpec(memory_space=pltpu.SMEM)]
        + [here] * 4
        + [there] * 4,
        out_specs=(here, here),
        scratch_shapes=[
            vmem((8 * HD, width), bf16),
            vmem((width, ff), bf16),
            vmem((width, ff), bf16),
            vmem((ff, width), bf16),
            vmem((96, 4, width), bf16),
            vmem((4, 96, 4, width), bf16),
            vmem((4, 96, 4, width), bf16),
            vmem((4, 2, 12, 4, width), bf16),
            vmem((4, 2, 12, 4, width), bf16),
            vmem((4, 2, 24, 4, width), bf16),
            vmem((4, 24, 4, width), bf16),
            vmem((96, 4, width), bf16),
            vmem((rows, width), bf16),
            vmem((rows, ff), bf16),
            vmem((32, BLK, BLK), bf16),
            vmem((32, BLK // 2, BLK), bf16),
            vmem((2, 4 * BLK, 256), bf16),
            vmem((2, 4 * BLK, HD), f32),
            vmem((2, 4 * BLK, 128), f32),
            vmem((BLK, BLK), bf16),
            vmem((BLK, 8 * HD), bf16),
            vmem((4, BLK // 4, width), bf16),
            vmem((3, BLK // 4, width), bf16),
            dma((4,)),
            dma,
            dma((4,)),
            dma((4, 2)),
            dma((4, 2)),
            dma((4, 2)),
            dma((4, 2)),
            dma((4, 2)),
            dma((4, 2)),
            dma((4, 2)),
            dma((4, 2)),
            dma((4, 4)),
            dma,
            dma((4,)),
            dma((3, 2)),
            dma((3, 2)),
            dma((3, 2)),
            dma((3, 2)),
            dma((4, 2)),
            dma((4, 2)),
            dma((3,)),
            dma((3,)),
            vmem((BLK, 8 * HD), bf16),
            vmem((4 * BLK, 2 * HD), bf16),
            vmem((4 * BLK, 2 * HD), bf16),
            dma((2,)),
            dma((2,)),
            vmem((4, 24, 4, width), bf16),
            dma,
            dma,
        ],
        compiler_params=pltpu.CompilerParams(
            vmem_limit_bytes=63 * 1024 * 1024, collective_id=0, has_side_effects=True
        ),
        name="step",
    )(
        query_rows,
        key_rows,
        value_rows,
        key_bias.T,
        head_offset,
        expert_input,
        expert_gain[None, :],
        routes.T,
        route_weight.T,
        out_weight,
        gate_weight,
        up_weight,
        down_weight,
    )


def solution(mesh):
    return jax.shard_map(
        body,
        mesh=mesh,
        in_specs=(
            P("ep", "tp"),
            P("ep", "tp"),
            P("ep", "tp"),
            P("ep", "tp"),
            P("tp"),
            P("tp", None),
            P(("ep", "tp"), None),
            P(),
            P(("ep", "tp"), None),
            P(("ep", "tp"), None),
            P("ep", None, "tp"),
            P("ep", None, "tp"),
            P("ep", "tp", None),
        ),
        out_specs=(P(("ep", "tp"), None), P(("ep", "tp"), None)),
        check_vma=False,
    )
```
